32 devices in a mesh: sp: 16 (over z, y, x), tp: 2 (over core).
Axes of the slice: x: 2, y: 2, z: 4, core: 2. Of those that a mesh axis runs over, the one named last changes fastest.
Arguments:
- moe_input: bfloat16 [4096, 2048], P('sp'), may hold values from -6 to 6
- cotangent: bfloat16 [4096, 2048], P('sp'), may hold values from -6 to 6
- expert_ids: int32 [4096, 2], P('sp'), may hold values from 0 to 15, all different within a row; in each aligned block of 256 rows (0 to 255, 256 to 511, ...) at most 64 rows name the same one
- route_weight: float32 [4096, 2], P('sp'), may hold values from 0.05 to 0.6
- gate_proj: bfloat16 [16, 2048, 1024], P('sp', None, 'tp'), may hold values from -0.125 to 0.125
- up_proj: bfloat16 [16, 2048, 1024], P('sp', None, 'tp'), may hold values from -0.125 to 0.125
- down_proj: bfloat16 [16, 1024, 2048], P('sp', 'tp'), may hold values from -0.1875 to 0.1875
- out_weight: bfloat16 [2048, 2048], P(None, 'tp'), may hold values from -0.125 to 0.125
- recur_input: bfloat16 [4096, 2048], P('sp', 'tp'), may hold values from -6 to 6
- gate_input: bfloat16 [4096, 2048], P('sp', 'tp'), may hold values from -6 to 6
- states: float32 [4096, 2048], P('sp', 'tp'), may hold values from -6 to 6
- conv_taps: bfloat16 [4, 2048], P(None, 'tp'), may hold values from -3 to 3
- decay_gate_w: bfloat16 [16, 128, 128], P('tp'), may hold values from -0.5 to 0.5
- input_gate_w: bfloat16 [16, 128, 128], P('tp'), may hold values from -0.5 to 0.5
- decay_rate: float32 [2048], P('tp'), may hold values from 7.3242187e-06 to 0.008
- decay_extra: float32 [4096, 2048], P('sp', 'tp'), may hold values from -0.77 to 0
Outputs:
- gate_proj_grad: bfloat16 [16, 2048, 1024], P('sp', None, 'tp')
- up_proj_grad: bfloat16 [16, 2048, 1024], P('sp', None, 'tp')
- down_proj_grad: bfloat16 [16, 1024, 2048], P('sp', 'tp')
- out_weight_grad: float32 [2048, 2048], P('sp', 'tp')
- input_grad: bfloat16 [4096, 2048], P('sp')
- recur_grad: bfloat16 [4096, 2048], P('sp', 'tp')
- gate_grad: bfloat16 [4096, 2048], P('sp', 'tp')
The draws below stay inside these ranges and needn't reach their ends.
Inputs may be any that keep to these rules, and one draw needn't show every extreme that they name: `expert_ids`: within each aligned block of 256 tokens a token names 2 different experts, and no expert is named more than 64 times.
All inputs are finite; a program needn't handle non-finite values.
Results may differ from the reference program's by a relative error of at most 0.012.
Values may be sent and summed in bfloat16 or wider, within the bound.
A program may use at most 128 MiB of HBM per device.

```python
import math
import jax
import jax.numpy as jnp
import numpy as np
from jax import lax

D = 2048
FF = 1024
RECURRENCE_WIDTH = 2048
LRU_BLOCKS = 16
TOPK = 2
TOK_DEV = 256
BLK = 128
SEQUENCE_TOKENS = 4096
EXPERTS = 16
CAP = 64
N_SP = 16
N_TP = 2


def decay_parts(key):
    base_key = jax.random.fold_in(key, 4242)
    multiple_count = jax.random.split(base_key, 6)
    fast_share = 0.5
    fast_mask = jax.random.uniform(multiple_count[0], (RECURRENCE_WIDTH,), jnp.float32) < fast_share
    slow_rate = jnp.exp(jax.random.uniform(multiple_count[1], (RECURRENCE_WIDTH,), jnp.float32, math.log(0.03 / SEQUENCE_TOKENS), math.log(0.15 / SEQUENCE_TOKENS)))
    fast_rate = jnp.exp(jax.random.uniform(multiple_count[2], (RECURRENCE_WIDTH,), jnp.float32, math.log(0.0025), math.log(0.008)))
    rate_value = jnp.where(fast_mask, fast_rate, slow_rate)
    block_count = SEQUENCE_TOKENS // TOK_DEV
    factor = jax.random.uniform(multiple_count[3], (block_count, RECURRENCE_WIDTH), jnp.float32, 0.0, 2.0)
    gentle_component = jnp.repeat(-4.0 * rate_value[None, :] * factor, TOK_DEV, axis=0)
    spike_indicator = jax.random.uniform(multiple_count[4], (SEQUENCE_TOKENS, RECURRENCE_WIDTH), jnp.float32) < 3.0 / SEQUENCE_TOKENS
    spike_magnitude = jax.random.uniform(multiple_count[5], (SEQUENCE_TOKENS, RECURRENCE_WIDTH), jnp.float32, 0.22, 0.7)
    additional_value = gentle_component - jnp.where(spike_indicator, spike_magnitude, 0.0)
    return (rate_value, additional_value)


def draw_decay_rate(key, part):
    return decay_parts(key)[0]


def draw_decay_extra(key, part):
    return decay_parts(key)[1]


def with_spikes(drawn, own_key, source, target, blocks, factor):
    def block_of(axis_at):
        return (jnp.arange(drawn.shape[axis_at]) // (drawn.shape[axis_at] // blocks)).reshape((-1,) + (1,) * (drawn.ndim - 1 - axis_at))

    near = jax.random.permutation(own_key, blocks)[block_of(target)]
    second = (block_of(target) + blocks // 2) % blocks
    return jnp.where((block_of(source) == near) | (block_of(source) == second), factor * drawn, drawn)


def levels(key, shape, shards, low, high):
    def one(axis_at, shards_of):
        draws = jax.random.uniform(jax.random.fold_in(jax.random.fold_in(key, 6), axis_at), (shards_of,), jnp.float32, low / len(shards), high / len(shards))
        return jnp.repeat(jnp.exp(draws), shape[axis_at] // shards_of).reshape((-1,) + (1,) * (len(shape) - axis_at - 1))

    loudness = one(*shards[0])
    for cut in shards[1:]:
        loudness = loudness * one(*cut)
    return loudness


def shared_out(own_key, own, number, rows, count, top, limit, lean):
    order = jax.random.permutation(own_key, count)
    heavy_load, ordinary = shares(count, rows * top, limit, lean, True), shares(count, rows * top, limit, lean, False)
    places = jnp.arange(count)

    def named(sizes, turn):
        used = int((sizes > 0).sum())
        fixed = max(1, used // 4)
        passed = fixed + (places - fixed + turn * (used - fixed)) % max(1, count - fixed)
        return jnp.zeros((count,), jnp.int32).at[order[jnp.where(places < fixed, places, passed)]].set(jnp.asarray(sizes, jnp.int32))

    sizes = jnp.where(number % 4 == 0, named(heavy_load, number // 4), named(ordinary, number - number // 4 - 1))
    mixed = jax.random.permutation(jax.random.fold_in(own, 3), count)
    donor, taker = mixed[0:count // 2 * 2:2], mixed[1:count // 2 * 2:2]
    margin = jnp.minimum(sizes[donor] - 1, limit - sizes[taker]) // 2
    margin = jnp.where((donor == order[0]) | (taker == order[0]) | (sizes[taker] == 0), 0, jnp.maximum(margin, 0))
    passed = jax.random.randint(jax.random.fold_in(own, 4), (count // 2,), 0, 1 << 20) % (margin + 1)
    sizes = sizes.at[donor].add(-passed).at[taker].add(passed)
    items = jnp.searchsorted(jnp.cumsum(sizes), jnp.arange(rows * top), side="right").astype(jnp.int32)
    grid = items.reshape(top, rows).T
    grid = grid[jax.random.permutation(jax.random.fold_in(own, 1), rows)]
    turn = jax.random.randint(jax.random.fold_in(own, 2), (rows, 1), 0, top)
    return jnp.take_along_axis(grid, (jnp.arange(top)[None, :] + turn) % top, axis=1)


def shares(amount, total, limit, lean, full):
    loads = [(1 << 20) // math.isqrt(rank ** lean) + 1 for rank in range(1, amount + 1)]
    largest = limit if full else min(limit, max(-(-total // amount), total * loads[0] // sum(loads)))
    least = 1 if total - largest >= amount - 1 else 0
    holding, surplus = [largest] + [least] * (amount - 1), total - largest - least * (amount - 1)
    while surplus > 0:
        free = [i for i in range(1, amount) if holding[i] < largest] or [i for i in range(1, amount) if holding[i] < limit]
        whole, left = sum([loads[i] for i in free]), surplus
        for i in free:
            extra = min(limit - holding[i], max(1, left * loads[i] // whole), surplus)
            holding[i] = holding[i] + extra
            surplus = surplus - extra
    return np.array(holding)


def bell_draw(key, dims, width, reach, cuts=(), kind=jnp.bfloat16):
    entries = width * jax.random.normal(key, dims, jnp.float32)
    if cuts:
        entries = entries * levels(key, dims, cuts, -0.22, 0.18)
    return jnp.clip(entries, -reach, reach).astype(kind)


def heavy_noise(own_key, shape, deviation, most, pieces, heavy, kind=jnp.bfloat16):
    values = deviation * jax.random.normal(own_key, shape, jnp.float32)
    if pieces:
        values = values * levels(own_key, shape, pieces, -0.22, 0.18)
    return jnp.clip(with_spikes(values, jax.random.fold_in(own_key, 3), *heavy), -most, most).astype(kind)


def setup_inputs(seed: int = 0) -> dict:
    keys = jax.random.split(jax.random.key(seed), 17)
    moe_input = bell_draw(keys[0], (SEQUENCE_TOKENS, D), 1.0, 6.0, ((0, 16),))
    cotangent = heavy_noise(keys[1], (SEQUENCE_TOKENS, D), 1.0, 6.0, ((0, 16),), (0, 1, 16, 2.0))
    expert_ids_keys = jax.random.split(jax.random.fold_in(keys[2], 1), SEQUENCE_TOKENS // TOK_DEV)
    expert_ids_turns = jax.random.permutation(jax.random.fold_in(keys[2], 3), SEQUENCE_TOKENS // TOK_DEV)
    expert_ids = jax.vmap(lambda own, number: shared_out(jax.random.fold_in(keys[2], 2), own, number, TOK_DEV, EXPERTS, TOPK, CAP, 1))(expert_ids_keys, expert_ids_turns).reshape((SEQUENCE_TOKENS, TOPK))
    route_weight = jnp.clip(0.05 + 0.55 * jax.random.uniform(keys[3], (SEQUENCE_TOKENS, TOPK), jnp.float32) ** levels(keys[3], (SEQUENCE_TOKENS, TOPK), ((0, 16),), -0.2, 0.2), 0.05, 0.6)
    gate_proj = bell_draw(keys[4], (EXPERTS, D, FF), D ** -0.5, 0.125, ((0, 16), (2, 2)))
    up_proj = bell_draw(keys[5], (EXPERTS, D, FF), D ** -0.5, 0.125, ((0, 16), (2, 2)))
    down_proj = bell_draw(keys[6], (EXPERTS, FF, D), FF ** -0.5, 0.1875, ((0, 16), (1, 2)))
    out_weight = bell_draw(keys[7], (D, RECURRENCE_WIDTH), RECURRENCE_WIDTH ** -0.5, 0.125, ((1, 2),))
    recur_input = bell_draw(keys[8], (SEQUENCE_TOKENS, RECURRENCE_WIDTH), 1.0, 6.0, ((0, 16), (1, 2)))
    gate_input = bell_draw(keys[9], (SEQUENCE_TOKENS, RECURRENCE_WIDTH), 1.0, 6.0, ((0, 16), (1, 2)))
    states = bell_draw(keys[10], (SEQUENCE_TOKENS, RECURRENCE_WIDTH), 1.0, 6.0, ((0, 16), (1, 2)), jnp.float32)
    conv_taps = bell_draw(keys[11], (4, RECURRENCE_WIDTH), 4 ** -0.5, 3.0, ((1, 2),))
    decay_gate_w = bell_draw(keys[12], (LRU_BLOCKS, BLK, BLK), BLK ** -0.5, 0.5, ((0, 2),))
    input_gate_w = bell_draw(keys[13], (LRU_BLOCKS, BLK, BLK), BLK ** -0.5, 0.5, ((0, 2),))
    decay_rate = draw_decay_rate(jax.random.fold_in(keys[16], 71), 0)
    decay_extra = draw_decay_extra(jax.random.fold_in(keys[16], 71), 0)
    return dict(moe_input=moe_input, cotangent=cotangent, expert_ids=expert_ids, route_weight=route_weight, gate_proj=gate_proj, up_proj=up_proj, down_proj=down_proj, out_weight=out_weight, recur_input=recur_input, gate_input=gate_input, states=states, conv_taps=conv_taps, decay_gate_w=decay_gate_w, input_gate_w=input_gate_w, decay_rate=decay_rate, decay_extra=decay_extra)


decay_scale = 8.0

def pair_combine(earlier, later):
    return (earlier[0] * later[0], later[0] * earlier[1] + later[1])

def rounded(value):
    return lax.optimization_barrier(value.astype(jnp.bfloat16)).astype(jnp.float32)

def slot_layout(expert_ids):
    source_ids = expert_ids.reshape(N_SP, TOK_DEV * TOPK)
    onehot = (source_ids[:, :, None] == jnp.arange(EXPERTS, dtype=jnp.int32)[None, None, :]).astype(jnp.int32)
    slot_rank = lax.optimization_barrier(jnp.sum((jnp.cumsum(onehot, axis=1) - onehot) * onehot, axis=2))
    sources = jnp.arange(N_SP, dtype=jnp.int32)[:, None]
    target = ((source_ids * N_SP + sources) * CAP + slot_rank).reshape(-1).astype(jnp.int32)
    source_table = jnp.full((EXPERTS * N_SP * CAP,), SEQUENCE_TOKENS * TOPK, jnp.int32)
    source_table = source_table.at[target].set(jnp.arange(SEQUENCE_TOKENS * TOPK, dtype=jnp.int32))
    return (source_table.reshape(EXPERTS, N_SP * CAP), target)

def reference(moe_input, cotangent, expert_ids, route_weight, gate_proj, up_proj, down_proj, out_weight, recur_input, gate_input, states, conv_taps, decay_gate_w, input_gate_w, decay_rate, decay_extra):
    cot_float = cotangent.astype(jnp.float32)
    scaled = (route_weight[:, :, None] * cot_float[:, None, :]).astype(jnp.bfloat16).reshape(SEQUENCE_TOKENS * TOPK, D)
    token_rows = jnp.repeat(moe_input, TOPK, axis=0)
    zero_row = jnp.zeros((1, D), jnp.bfloat16)
    padded_rows = jnp.concatenate([token_rows, zero_row], axis=0)
    padded_cot = jnp.concatenate([scaled, zero_row], axis=0)
    source_table, target = slot_layout(expert_ids)

    def one_expert(inputs):
        slot_index, weight_gate, weight_up, weight_down = inputs
        rows_float = padded_rows[slot_index].astype(jnp.float32)
        cot_rows = padded_cot[slot_index].astype(jnp.float32)
        gate_float = weight_gate.astype(jnp.float32)
        up_float = weight_up.astype(jnp.float32)
        down_float = weight_down.astype(jnp.float32)
        gate_pre = jnp.dot(rows_float, gate_float)
        up_pre = jnp.dot(rows_float, up_float)
        sigmoid_gate = jax.nn.sigmoid(gate_pre)
        silu_gate = gate_pre * sigmoid_gate
        hidden = rounded(silu_gate * up_pre)
        down_grad = jnp.dot(hidden.T, cot_rows)
        hidden_grad = jnp.dot(cot_rows, down_float.T)
        gate_pre_grad = rounded(hidden_grad * up_pre * sigmoid_gate * (1.0 + gate_pre * (1.0 - sigmoid_gate)))
        up_pre_grad = rounded(hidden_grad * silu_gate)
        gate_weight_grad = jnp.dot(rows_float.T, gate_pre_grad)
        up_weight_grad = jnp.dot(rows_float.T, up_pre_grad)
        share_size = FF // N_TP
        summed = jnp.zeros((N_SP * CAP, D), jnp.float32)
        for part_index in range(N_TP):
            lower = part_index * share_size
            upper = lower + share_size
            piece_grad = jnp.dot(gate_pre_grad[:, lower:upper], gate_float[:, lower:upper].T) + jnp.dot(up_pre_grad[:, lower:upper], up_float[:, lower:upper].T)
            summed = summed + rounded(piece_grad)
        return (gate_weight_grad.astype(jnp.bfloat16), up_weight_grad.astype(jnp.bfloat16), down_grad.astype(jnp.bfloat16), summed.astype(jnp.bfloat16))
    gate_proj_grad, up_proj_grad, down_proj_grad, slot_grad = lax.map(one_expert, (source_table, gate_proj, up_proj, down_proj))
    gathered = slot_grad.reshape(EXPERTS * N_SP * CAP, D)[target].astype(jnp.float32)
    gathered = gathered.reshape(SEQUENCE_TOKENS, TOPK, D)
    moe_grad = gathered[:, 0]
    for choice_index in range(1, TOPK):
        moe_grad = moe_grad + gathered[:, choice_index]
    input_grad = (moe_grad + cot_float).astype(jnp.bfloat16)
    grad_float = input_grad.astype(jnp.float32)
    gate_float_in = gate_input.astype(jnp.float32)
    gelu_value, gelu_back = jax.vjp(jax.nn.gelu, gate_float_in)
    mixer_out = (states * gelu_value).astype(jnp.bfloat16).astype(jnp.float32)
    out_weight_grad = jnp.dot(grad_float.T, mixer_out)
    mixer_grad = jnp.dot(grad_float, out_weight.astype(jnp.float32))
    gate_grad = gelu_back(mixer_grad * states)[0].astype(jnp.bfloat16)
    state_grad = mixer_grad * gelu_value
    taps = conv_taps.astype(jnp.float32)
    padded_in = jnp.pad(recur_input.astype(jnp.float32), ((3, 0), (0, 0)))
    conv = taps[0] * padded_in[0:SEQUENCE_TOKENS]
    for tap_index in range(1, 4):
        conv = conv + taps[tap_index] * padded_in[tap_index:tap_index + SEQUENCE_TOKENS]
    conv_blocks = rounded(conv).reshape(SEQUENCE_TOKENS, LRU_BLOCKS, BLK)
    decay_w = decay_gate_w.astype(jnp.float32)
    input_w = input_gate_w.astype(jnp.float32)
    decay_pre = jnp.einsum('tbi,bij->tbj', conv_blocks, decay_w).reshape(SEQUENCE_TOKENS, RECURRENCE_WIDTH)
    input_pre = jnp.einsum('tbi,bij->tbj', conv_blocks, input_w).reshape(SEQUENCE_TOKENS, RECURRENCE_WIDTH)
    recur_gate = jax.nn.sigmoid(decay_pre)
    input_gate = jax.nn.sigmoid(input_pre)
    positions = jnp.arange(SEQUENCE_TOKENS, dtype=jnp.int32)
    first_row = (positions == 0)[:, None]
    log_decay = -decay_scale * recur_gate * decay_rate[None, :] + decay_extra
    decay_value = jnp.exp(log_decay)
    mult = jnp.where(first_row, 1.0, jnp.sqrt(-jnp.expm1(2.0 * log_decay)))
    prev_states = jnp.concatenate([jnp.zeros((1, RECURRENCE_WIDTH), jnp.float32), states[:-1]], axis=0)
    next_decay = jnp.concatenate([decay_value[1:], jnp.zeros((1, RECURRENCE_WIDTH), jnp.float32)], axis=0)
    cumul_flip, values_flip = lax.associative_scan(pair_combine, (next_decay[::-1], state_grad[::-1]), axis=0)
    carried_grad = values_flip[::-1]
    log_grad = carried_grad * prev_states * decay_value - jnp.where(first_row, 0.0, carried_grad * input_gate * conv * decay_value * decay_value / mult)
    decay_pre_grad = rounded(log_grad * (-decay_scale * decay_rate[None, :]) * recur_gate * (1.0 - recur_gate))
    input_pre_grad = rounded(carried_grad * mult * conv * input_gate * (1.0 - input_gate))
    conv_grad = carried_grad * mult * input_gate + jnp.einsum('tbj,bij->tbi', decay_pre_grad.reshape(SEQUENCE_TOKENS, LRU_BLOCKS, BLK), decay_w).reshape(SEQUENCE_TOKENS, RECURRENCE_WIDTH) + jnp.einsum('tbj,bij->tbi', input_pre_grad.reshape(SEQUENCE_TOKENS, LRU_BLOCKS, BLK), input_w).reshape(SEQUENCE_TOKENS, RECURRENCE_WIDTH)
    padded_grad = jnp.pad(conv_grad, ((0, 3), (0, 0)))
    recur_float = taps[0] * padded_grad[3:3 + SEQUENCE_TOKENS]
    for tap_index in range(1, 4):
        recur_float = recur_float + taps[tap_index] * padded_grad[3 - tap_index:3 - tap_index + SEQUENCE_TOKENS]
    recur_grad = recur_float.astype(jnp.bfloat16)
    return (gate_proj_grad, up_proj_grad, down_proj_grad, out_weight_grad, input_grad, recur_grad, gate_grad)
```

```python
import functools

import jax
import jax.numpy as jnp
from jax import lax
from jax.experimental import pallas as pl
from jax.experimental.pallas import tpu as pltpu
from jax.sharding import PartitionSpec as P

decay_scale = 8.0
BF = jnp.bfloat16
F32 = jnp.float32
PLANES = 4
MESH = pl.DeviceIdType.MESH


def dot_nn(left, right):
    return jnp.dot(left, right, preferred_element_type=F32)


def dot_nt(left, right):
    return lax.dot_general(left, right, (((1,), (1,)), ((), ())), preferred_element_type=F32)


def dot_tn(left, right):
    return lax.dot_general(left, right, (((0,), (0,)), ((), ())), preferred_element_type=F32)


def aligned(index, size):
    return pl.ds(pl.multiple_of(index * size, size), size)


def local_wait(view, sem):
    pltpu.make_async_copy(view, view, sem).wait()


def remote(src, dst, send, recv, **where):
    return pltpu.make_async_remote_copy(
        src_ref=src, dst_ref=dst, send_sem=send, recv_sem=recv, device_id=where, device_id_type=MESH
    )


def expert_kernel(
    count, cap,
    tok_ref, cot_ref, place_ref, place_t_ref, weight_ref, mixer_ref, gate_w, up_w, down_w,
    grad_ref, plane_ref, gate_g, up_g, down_g,
    wgu, wd, send_r, send_g, rows, grads, pre, hid, xgu, own, psend, precv, tsend, back, halves,
    dgu, ddown,
    load_sem, bulk_sem, rows_sem, grads_sem, back_sem, mixer_sem, pair_send, pair_recv,
):
    me, core = lax.axis_index("sp"), lax.axis_index("tp")
    other = 1 - core
    peers = count // PLANES
    zed, pos = me // peers, lax.rem(me, peers)
    group = peers * cap
    tokens, width = tok_ref.shape
    half = width // 2
    hidden = wd.shape[0]
    mine = aligned(core, half)
    theirs = aligned(other, half)

    loads = [
        pltpu.make_async_copy(gate_w, wgu.at[:, pl.ds(0, hidden)], load_sem.at[0]),
        pltpu.make_async_copy(up_w, wgu.at[:, pl.ds(hidden, hidden)], load_sem.at[1]),
        pltpu.make_async_copy(down_w, wd, load_sem.at[2]),
    ]
    for load in loads:
        load.start()

    barrier = pltpu.get_barrier_semaphore()

    def greet(step, carry):
        pl.semaphore_signal(
            barrier, inc=1, device_id={"sp": lax.rem(me + step, count)}, device_id_type=MESH
        )
        return carry

    lax.fori_loop(1, count, greet, 0)
    pl.semaphore_signal(barrier, inc=1, device_id={"tp": other}, device_id_type=MESH)

    def place(step, source, scaled):
        plane = lax.rem(zed + (PLANES - 1 - step), PLANES)
        span = aligned(plane, group)
        placed = dot_nn(place_ref[span, :], source[:, mine])
        if scaled:
            placed = placed * weight_ref[span, :]
        return plane, span, placed.astype(BF)

    def spread(step, plane, source, target, which, sems):
        def one(shift, carry):
            dest = plane * peers + lax.rem(pos + shift, peers)
            remote(
                source.at[aligned(dest, cap)], target.at[aligned(me, cap)],
                bulk_sem.at[which], sems.at[zed], sp=dest,
            ).start()
            return carry

        lax.fori_loop(jnp.where(step == PLANES - 1, 1, 0), peers, one, 0)

        @pl.when(step == PLANES - 1)
        def _():
            pltpu.make_async_copy(
                source.at[aligned(me, cap)], target.at[aligned(me, cap)], sems.at[zed]
            ).start()

    for which, (source, sent, target, sems) in enumerate(
        ((tok_ref, send_r, rows, rows_sem), (cot_ref, send_g, grads, grads_sem))
    ):
        def issue(step, carry, which=which, source=source, sent=sent, target=target, sems=sems):
            plane, span, placed = place(step, source, which == 1)
            sent[span, :] = placed
            if which == 0:
                @pl.when(step == 0)
                def _():
                    pl.semaphore_wait(barrier, count)
            spread(step, plane, sent, target.at[core], which, sems)
            return carry

        lax.fori_loop(0, PLANES, issue, 0)

    def share(shift, carry):
        dest = zed * peers + lax.rem(pos + shift, peers)
        remote(
            mixer_ref, plane_ref.at[aligned(pos, tokens)], bulk_sem.at[3], mixer_sem.at[0], sp=dest
        ).start()
        return carry

    lax.fori_loop(1, peers, share, 0)
    keep = pltpu.make_async_copy(mixer_ref, plane_ref.at[aligned(pos, tokens)], mixer_sem.at[1])
    keep.start()

    def from_plane(step):
        return lax.rem(zed + step + 1, PLANES)

    def to_pair(view, slot):
        return remote(view, view, pair_send.at[slot], pair_recv.at[slot], tp=other)

    def pass_rows(step, carry):
        span = aligned(from_plane(step), group)
        view = rows.at[core, span]
        local_wait(view, rows_sem.at[from_plane(step)])
        to_pair(view, step).start()
        return carry

    lax.fori_loop(0, PLANES, pass_rows, 0)
    for load in loads:
        load.wait()

    def forward(step, carry):
        span = aligned(from_plane(step), group)
        to_pair(rows.at[other, span], step).wait_recv()
        pre[span, :] = dot_nn(rows[0, span, :], wgu[:half, :]) + dot_nn(
            rows[1, span, :], wgu[half:, :]
        )
        return carry

    lax.fori_loop(0, PLANES, forward, 0)

    def finish(step):
        plane = from_plane(step)
        span = aligned(plane, group)
        to_pair(precv.at[span], 2 * PLANES + step).wait_recv()
        tsend[span, :] = (own[lax.rem(step, 2)] + precv[span, :].astype(F32)).astype(BF)

        def one(shift, carry):
            dest = plane * peers + lax.rem(pos + shift, peers)
            remote(
                tsend.at[aligned(dest, cap)], back.at[aligned(me, cap)],
                bulk_sem.at[2], back_sem.at[zed], sp=dest,
            ).start()
            return carry

        lax.fori_loop(jnp.where(step == PLANES - 1, 1, 0), peers, one, 0)

        @pl.when(step == PLANES - 1)
        def _():
            pltpu.make_async_copy(
                tsend.at[aligned(me, cap)], back.at[aligned(me, cap)], back_sem.at[zed]
            ).start()

    def backward(step, carry):
        plane = from_plane(step)
        span = aligned(plane, group)
        view = grads.at[core, span]
        local_wait(view, grads_sem.at[plane])
        to_pair(view, PLANES + step).start()

        @pl.when(step > 0)
        def _():
            finish(step - 1)

        to_pair(grads.at[other, span], PLANES + step).wait_recv()
        hidden_grad = dot_nt(grads[0, span, :], wd[:, :half]) + dot_nt(
            grads[1, span, :], wd[:, half:]
        )
        gate = pre[span, :hidden]
        up = pre[span, hidden:]
        sig = jax.nn.sigmoid(gate)
        silu = gate * sig
        hid[span, :] = (silu * up).astype(BF)
        xgu[span, :hidden] = (hidden_grad * up * sig * (1.0 + gate * (1.0 - sig))).astype(BF)
        xgu[span, hidden:] = (hidden_grad * silu).astype(BF)
        psend[span, :] = dot_nt(xgu[span, :], wgu[theirs, :]).astype(BF)
        remote(
            psend.at[span], precv.at[span], pair_send.at[2 * PLANES + step],
            pair_recv.at[2 * PLANES + step], tp=other,
        ).start()
        own[lax.rem(step, 2)] = dot_nt(xgu[span, :], wgu[mine, :])
        return carry

    lax.fori_loop(0, PLANES, backward, 0)
    finish(PLANES - 1)

    tile = 256
    tiles = half // tile

    for side in range(2):
        def weight_tile(step, carry, side=side):
            columns = aligned(step, tile)
            spot = pl.ds(pl.multiple_of(side * half + step * tile, tile), tile)
            dgu[spot, :] = dot_tn(rows[side, :, columns], xgu[...]).astype(BF)
            ddown[:, spot] = dot_tn(hid[...], grads[side, :, columns]).astype(BF)
            return carry

        lax.fori_loop(0, tiles, weight_tile, 0)

    stores = [
        pltpu.make_async_copy(dgu.at[:, pl.ds(0, hidden)], gate_g, load_sem.at[0]),
        pltpu.make_async_copy(dgu.at[:, pl.ds(hidden, hidden)], up_g, load_sem.at[1]),
        pltpu.make_async_copy(ddown, down_g, load_sem.at[2]),
    ]
    for store in stores:
        store.start()

    def gather(step, carry):
        plane = from_plane(step)
        local_wait(back.at[aligned(plane, group)], back_sem.at[plane])
        return carry

    lax.fori_loop(0, PLANES, gather, 0)
    moe = dot_nn(place_t_ref[...], back[...])
    halves[core] = (moe + cot_ref[:, mine].astype(F32)).astype(BF)
    last = to_pair(halves.at[core], 3 * PLANES)
    last.start()
    grad_ref[:, mine] = halves[core]
    to_pair(halves.at[other], 3 * PLANES).wait_recv()
    grad_ref[:, theirs] = halves[other]

    sent_rows = (count - 1) * cap
    for which in range(3):
        local_wait(send_r.at[pl.ds(0, sent_rows)], bulk_sem.at[which])
    shared = plane_ref.at[pl.ds(0, (peers - 1) * tokens)]
    local_wait(shared, bulk_sem.at[3])
    local_wait(shared, mixer_sem.at[0])
    keep.wait()
    for slot in range(2 * PLANES):
        to_pair(rows.at[0, pl.ds(0, group)], slot).wait_send()
    for slot in range(2 * PLANES, 3 * PLANES):
        to_pair(psend.at[pl.ds(0, group)], slot).wait_send()
    last.wait_send()
    for store in stores:
        store.wait()


def expert_exchange(tok, cot, place, place_t, weight, mixer, gate_w, up_w, down_w):
    count = lax.axis_size("sp")
    tokens, width = tok.shape
    slots = place.shape[0]
    cap = slots // count
    half = width // 2
    hidden = gate_w.shape[1]
    peers = count // PLANES
    group = peers * cap
    vmem, anywhere = pl.BlockSpec(memory_space=pltpu.VMEM), pl.BlockSpec(memory_space=pl.ANY)
    dma = pltpu.SemaphoreType.DMA
    flops = 2 * slots * width * hidden * 8
    return pl.pallas_call(
        functools.partial(expert_kernel, count, cap),
        in_specs=[vmem] * 6 + [anywhere] * 3,
        out_specs=[vmem] + [anywhere] * 4,
        out_shape=[
            jax.ShapeDtypeStruct((tokens, width), BF),
            jax.ShapeDtypeStruct((peers * tokens, mixer.shape[1]), BF),
            jax.ShapeDtypeStruct(gate_w.shape, BF),
            jax.ShapeDtypeStruct(up_w.shape, BF),
            jax.ShapeDtypeStruct(down_w.shape, BF),
        ],
        scratch_shapes=[
            pltpu.VMEM((width, 2 * hidden), BF),
            pltpu.VMEM((hidden, width), BF),
            pltpu.VMEM((slots, half), BF),
            pltpu.VMEM((slots, half), BF),
            pltpu.VMEM((2, slots, half), BF),
            pltpu.VMEM((2, slots, half), BF),
            pltpu.VMEM((slots, 2 * hidden), F32),
            pltpu.VMEM((slots, hidden), BF),
            pltpu.VMEM((slots, 2 * hidden), BF),
            pltpu.VMEM((2, group, half), F32),
            pltpu.VMEM((slots, half), BF),
            pltpu.VMEM((slots, half), BF),
            pltpu.VMEM((slots, half), BF),
            pltpu.VMEM((slots, half), BF),
            pltpu.VMEM((2, tokens, half), BF),
            pltpu.VMEM((width, 2 * hidden), BF),
            pltpu.VMEM((hidden, width), BF),
            dma((3,)), dma((4,)), dma((PLANES,)), dma((PLANES,)), dma((PLANES,)), dma((2,)),
            dma((3 * PLANES + 1,)), dma((3 * PLANES + 1,)),
        ],
        compiler_params=pltpu.CompilerParams(
            collective_id=0, has_side_effects=True, vmem_limit_bytes=62 * 1024 * 1024
        ),
        cost_estimate=pl.CostEstimate(flops=flops, bytes_accessed=20 << 20, transcendentals=0),
        name="expert_exchange",
    )(tok, cot, place, place_t, weight, mixer, gate_w, up_w, down_w)


def passed_along(value, axis, steps):
    count = lax.axis_size(axis)
    initial, last = (max(0, -steps), min(count, count - steps))
    return lax.ppermute(value, axis, [(source, source + steps) for source in range(initial, last)])


def swapped(value, axis):
    return lax.ppermute(value, axis, [(0, 1), (1, 0)])


def carried_in(product, total, axis):
    count, mine = (lax.axis_size(axis), lax.axis_index(axis))
    pair = jnp.stack([product, total])
    pieces = lax.all_to_all(
        jnp.broadcast_to(pair[None], (count,) + pair.shape),
        axis,
        split_axis=0,
        concat_axis=0,
        tiled=True,
    )
    entering = jnp.zeros_like(total)
    for position in range(count - 1, 0, -1):
        longer = pieces[position, 0] * entering + pieces[position, 1]
        entering = jnp.where(position > mine, longer, entering)
    return entering


def scan_kernel(decay_ref, grad_ref, product_ref, local_ref):
    rows, lanes = decay_ref.shape
    group = 8
    last = rows // group - 1

    def step(index, carry):
        product, total, decay = carry
        start = pl.multiple_of((last - index) * group, group)
        decays = decay_ref[pl.ds(start, group), :]
        grads = grad_ref[pl.ds(start, group), :]
        products, totals = ([None] * group, [None] * group)
        for row in range(group - 1, -1, -1):
            product = product * decay
            total = grads[row : row + 1] + decay * total
            decay = decays[row : row + 1]
            products[row], totals[row] = (product, total)
        product_ref[pl.ds(start, group), :] = jnp.concatenate(products, axis=0)
        local_ref[pl.ds(start, group), :] = jnp.concatenate(totals, axis=0)
        return (product, total, decay)

    one = jnp.ones((1, lanes), jnp.float32)
    lax.fori_loop(0, last + 1, step, (one, jnp.zeros_like(one), one))


def reverse_scan(decay, grad):
    rows, channels = decay.shape
    width = 512 if channels % 512 == 0 else channels
    block = pl.BlockSpec((rows, width), lambda index: (0, index))
    return pl.pallas_call(
        scan_kernel,
        grid=(channels // width,),
        in_specs=[block, block],
        out_specs=[block, block],
        out_shape=[jax.ShapeDtypeStruct(decay.shape, jnp.float32)] * 2,
        cost_estimate=pl.CostEstimate(
            flops=3 * rows * channels, bytes_accessed=16 * rows * channels, transcendentals=0
        ),
        name="reverse_scan",
    )(decay, grad)


def contract_rows(left, right):
    return lax.dot_general(
        left, right, (((0,), (0,)), ((), ())), preferred_element_type=jnp.float32
    )


def contract_cols(left, right):
    return lax.dot_general(
        left, right, (((1,), (1,)), ((), ())), preferred_element_type=jnp.float32
    )


def on_device(
    moe_input,
    cotangent,
    expert_ids,
    route_weight,
    gate_proj,
    up_proj,
    down_proj,
    out_weight,
    recur_input,
    gate_input,
    states,
    conv_taps,
    decay_gate_w,
    input_gate_w,
    decay_rate,
    decay_extra,
):
    experts = lax.axis_size("sp")
    cores = lax.axis_size("tp")
    tok_rows, width = moe_input.shape
    top_count = expert_ids.shape[1]
    capacity = max(2, 4 * tok_rows // experts)
    slot_count = experts * capacity
    gate_float = gate_input.astype(jnp.float32)
    gelu_value, gelu_back = jax.vjp(jax.nn.gelu, gate_float)
    mixer_out = (states * gelu_value).astype(jnp.bfloat16)
    flat_ids = expert_ids.reshape(-1)
    onehot = (flat_ids[:, None] == jnp.arange(experts, dtype=jnp.int32)[None, :]).astype(jnp.int32)
    slot_rank = jnp.sum((jnp.cumsum(onehot, axis=0) - onehot) * onehot, axis=1)
    pair_slots = (flat_ids * capacity + slot_rank).reshape(tok_rows, top_count)
    slot_iota = jnp.arange(slot_count, dtype=jnp.int32)
    placing = slot_iota[:, None, None] == pair_slots[None, :, :]
    place = jnp.any(placing, axis=2).astype(jnp.bfloat16)
    place_t = jnp.any(pair_slots[:, :, None] == slot_iota[None, None, :], axis=1).astype(jnp.bfloat16)
    weight = jnp.sum(jnp.where(placing, route_weight[None], 0.0), axis=(1, 2))[:, None]
    input_grad, mixer_plane, gate_weight_grad, up_weight_grad, down_grad = expert_exchange(
        moe_input, cotangent, place, place_t, weight, mixer_out, gate_proj[0], up_proj[0], down_proj[0]
    )
    mixer_all = lax.all_gather(mixer_out, "sp", axis=0, tiled=True)
    column_share = width // experts
    grad_columns = lax.all_to_all(
        input_grad.reshape(tok_rows, experts, column_share).transpose(1, 0, 2),
        "sp",
        split_axis=0,
        concat_axis=0,
        tiled=True,
    ).reshape(experts * tok_rows, column_share)
    out_weight_grad = contract_rows(grad_columns, mixer_all)
    mixer_grad = jnp.dot(input_grad, out_weight, preferred_element_type=jnp.float32)
    gate_grad = gelu_back(mixer_grad * states)[0].astype(jnp.bfloat16)
    state_grad = mixer_grad * gelu_value
    channels = recur_input.shape[1]
    prev_inputs, prev_state = passed_along(
        (recur_input[-3:].astype(jnp.float32), states[-1:]), "sp", 1
    )
    extended = jnp.concatenate([prev_inputs, recur_input.astype(jnp.float32)], axis=0)
    taps = conv_taps.astype(jnp.float32)
    conv = taps[0] * extended[0:tok_rows]
    for tap_index in range(1, 4):
        conv = conv + taps[tap_index] * extended[tap_index : tap_index + tok_rows]
    blocks = decay_gate_w.shape[0]
    block_width = decay_gate_w.shape[1]
    conv_blocks = conv.astype(jnp.bfloat16).reshape(tok_rows, blocks, block_width)
    decay_pre = jnp.einsum(
        "tbi,bij->tbj", conv_blocks, decay_gate_w, preferred_element_type=jnp.float32
    ).reshape(tok_rows, channels)
    input_pre = jnp.einsum(
        "tbi,bij->tbj", conv_blocks, input_gate_w, preferred_element_type=jnp.float32
    ).reshape(tok_rows, channels)
    recur_gate = jax.nn.sigmoid(decay_pre)
    input_gate = jax.nn.sigmoid(input_pre)
    positions = lax.axis_index("sp") * tok_rows + jnp.arange(tok_rows, dtype=jnp.int32)
    first_row = (positions == 0)[:, None]
    log_decay = -decay_scale * recur_gate * decay_rate[None, :] + decay_extra
    decay_value = jnp.exp(log_decay)
    mult = jnp.where(first_row, 1.0, jnp.sqrt(-jnp.expm1(2.0 * log_decay)))
    prev_states = jnp.concatenate([prev_state, states[:-1]], axis=0)
    cumul, local_values = reverse_scan(decay_value, state_grad)
    entering = carried_in(decay_value[0] * cumul[0], decay_value[0] * local_values[0], "sp")
    carried_grad = local_values + cumul * entering[None, :]
    log_grad = carried_grad * prev_states * decay_value - jnp.where(
        first_row, 0.0, carried_grad * input_gate * conv * decay_value * decay_value / mult
    )
    decay_pre_grad = (
        log_grad * (-decay_scale * decay_rate[None, :]) * recur_gate * (1.0 - recur_gate)
    ).astype(jnp.bfloat16)
    input_pre_grad = (carried_grad * mult * conv * input_gate * (1.0 - input_gate)).astype(
        jnp.bfloat16
    )
    conv_grad = (
        carried_grad * mult * input_gate
        + jnp.einsum(
            "tbj,bij->tbi",
            decay_pre_grad.reshape(tok_rows, blocks, block_width),
            decay_gate_w,
            preferred_element_type=jnp.float32,
        ).reshape(tok_rows, channels)
        + jnp.einsum(
            "tbj,bij->tbi",
            input_pre_grad.reshape(tok_rows, blocks, block_width),
            input_gate_w,
            preferred_element_type=jnp.float32,
        ).reshape(tok_rows, channels)
    )
    next_grads = passed_along(conv_grad[:3], "sp", -1)
    grad_extended = jnp.concatenate([conv_grad, next_grads], axis=0)
    recur_float = taps[0] * grad_extended[3 : 3 + tok_rows]
    for tap_index in range(1, 4):
        recur_float = (
            recur_float + taps[tap_index] * grad_extended[3 - tap_index : 3 - tap_index + tok_rows]
        )
    recur_grad = recur_float.astype(jnp.bfloat16)
    return (
        gate_weight_grad.astype(jnp.bfloat16)[None],
        up_weight_grad.astype(jnp.bfloat16)[None],
        down_grad.astype(jnp.bfloat16)[None],
        out_weight_grad,
        input_grad,
        recur_grad,
        gate_grad,
    )


def solution(mesh):
    return jax.shard_map(
        on_device,
        mesh=mesh,
        in_specs=(
            P("sp", None),
            P("sp", None),
            P("sp", None),
            P("sp", None),
            P("sp", None, "tp"),
            P("sp", None, "tp"),
            P("sp", "tp", None),
            P(None, "tp"),
            P("sp", "tp"),
            P("sp", "tp"),
            P("sp", "tp"),
            P(None, "tp"),
            P("tp", None, None),
            P("tp", None, None),
            P("tp"),
            P("sp", "tp"),
        ),
        out_specs=(
            P("sp", None, "tp"),
            P("sp", None, "tp"),
            P("sp", "tp", None),
            P("sp", "tp"),
            P("sp", None),
            P("sp", "tp"),
            P("sp", "tp"),
        ),
        check_vma=False,
    )
```

```python
import functools

import jax
import jax.numpy as jnp
from jax import lax
from jax.experimental import pallas as pl
from jax.experimental.pallas import tpu as pltpu
from jax.sharding import PartitionSpec as P

decay_scale = 8.0
BF = jnp.bfloat16
F32 = jnp.float32
PLANES = 4
MESH = pl.DeviceIdType.MESH


def dot_nn(left, right):
    return jnp.dot(left, right, preferred_element_type=F32)


def dot_nt(left, right):
    return lax.dot_general(left, right, (((1,), (1,)), ((), ())), preferred_element_type=F32)


def dot_tn(left, right):
    return lax.dot_general(left, right, (((0,), (0,)), ((), ())), preferred_element_type=F32)


def aligned(index, size):
    return pl.ds(pl.multiple_of(index * size, size), size)


def local_wait(view, sem):
    pltpu.make_async_copy(view, view, sem).wait()


def remote(src, dst, send, recv, **where):
    return pltpu.make_async_remote_copy(
        src_ref=src, dst_ref=dst, send_sem=send, recv_sem=recv, device_id=where, device_id_type=MESH
    )


def expert_kernel(
    count, cap,
    tok_ref, cot_ref, place_ref, place_t_ref, weight_ref, mixer_ref, gate_w, up_w, down_w,
    grad_ref, plane_ref, gate_g, up_g, down_g,
    wgu, wd, send_r, send_g, rows, grads, pre, hid, xgu, own, psend, precv, tsend, back, halves,
    dgu, ddown,
    load_sem, bulk_sem, rows_sem, grads_sem, back_sem, mixer_sem, pair_send, pair_recv,
):
    me, core = lax.axis_index("sp"), lax.axis_index("tp")
    other = 1 - core
    peers = count // PLANES
    zed, pos = me // peers, lax.rem(me, peers)
    group = peers * cap
    tokens, width = tok_ref.shape
    half = width // 2
    hidden = wd.shape[0]
    mine = aligned(core, half)
    theirs = aligned(other, half)

    loads = [
        pltpu.make_async_copy(gate_w, wgu.at[:, pl.ds(0, hidden)], load_sem.at[0]),
        pltpu.make_async_copy(up_w, wgu.at[:, pl.ds(hidden, hidden)], load_sem.at[1]),
        pltpu.make_async_copy(down_w, wd, load_sem.at[2]),
    ]
    for load in loads:
        load.start()

    barrier = pltpu.get_barrier_semaphore()

    def greet(step, carry):
        pl.semaphore_signal(
            barrier, inc=1, device_id={"sp": lax.rem(me + step, count)}, device_id_type=MESH
        )
        return carry

    lax.fori_loop(1, count, greet, 0)
    pl.semaphore_signal(barrier, inc=1, device_id={"tp": other}, device_id_type=MESH)

    def place(step, source, scaled):
        plane = lax.rem(zed + (PLANES - 1 - step), PLANES)
        span = aligned(plane, group)
        placed = dot_nn(place_ref[span, :], source[:, mine])
        if scaled:
            placed = placed * weight_ref[span, :]
        return plane, span, placed.astype(BF)

    def spread(step, plane, source, target, which, sems):
        def one(shift, carry):
            dest = plane * peers + lax.rem(pos + shift, peers)
            remote(
                source.at[aligned(dest, cap)], target.at[aligned(me, cap)],
                bulk_sem.at[which], sems.at[zed], sp=dest,
            ).start()
            return carry

        lax.fori_loop(jnp.where(step == PLANES - 1, 1, 0), peers, one, 0)

        @pl.when(step == PLANES - 1)
        def _():
            pltpu.make_async_copy(
                source.at[aligned(me, cap)], target.at[aligned(me, cap)], sems.at[zed]
            ).start()

    for which, (source, sent, target, sems) in enumerate(
        ((tok_ref, send_r, rows, rows_sem), (cot_ref, send_g, grads, grads_sem))
    ):
        def issue(step, carry, which=which, source=source, sent=sent, target=target, sems=sems):
            plane, span, placed = place(step, source, which == 1)
            sent[span, :] = placed
            if which == 0:
                @pl.when(step == 0)
                def _():
                    pl.semaphore_wait(barrier, count)
            spread(step, plane, sent, target.at[core], which, sems)
            return carry

        lax.fori_loop(0, PLANES, issue, 0)

    def share(shift, carry):
        dest = zed * peers + lax.rem(pos + shift, peers)
        remote(
            mixer_ref, plane_ref.at[aligned(pos, tokens)], bulk_sem.at[3], mixer_sem.at[0], sp=dest
        ).start()
        return carry

    lax.fori_loop(1, peers, share, 0)
    keep = pltpu.make_async_copy(mixer_ref, plane_ref.at[aligned(pos, tokens)], mixer_sem.at[1])
    keep.start()

    def from_plane(step):
        return lax.rem(zed + step + 1, PLANES)

    def to_pair(view, slot):
        return remote(view, view, pair_send.at[slot], pair_recv.at[slot], tp=other)

    def pass_rows(step, carry):
        span = aligned(from_plane(step), group)
        view = rows.at[core, span]
        local_wait(view, rows_sem.at[from_plane(step)])
        to_pair(view, step).start()
        return carry

    lax.fori_loop(0, PLANES, pass_rows, 0)
    for load in loads:
        load.wait()

    def forward(step, carry):
        span = aligned(from_plane(step), group)
        to_pair(rows.at[other, span], step).wait_recv()
        pre[span, :] = dot_nn(rows[0, span, :], wgu[:half, :]) + dot_nn(
            rows[1, span, :], wgu[half:, :]
        )
        return carry

    lax.fori_loop(0, PLANES, forward, 0)

    def finish(step):
        plane = from_plane(step)
        span = aligned(plane, group)
        to_pair(precv.at[span], 2 * PLANES + step).wait_recv()
        tsend[span, :] = (own[lax.rem(step, 2)] + precv[span, :].astype(F32)).astype(BF)

        def one(shift, carry):
            dest = plane * peers + lax.rem(pos + shift, peers)
            remote(
                tsend.at[aligned(dest, cap)], back.at[aligned(me, cap)],
                bulk_sem.at[2], back_sem.at[zed], sp=dest,
            ).start()
            return carry

        lax.fori_loop(jnp.where(step == PLANES - 1, 1, 0), peers, one, 0)

        @pl.when(step == PLANES - 1)
        def _():
            pltpu.make_async_copy(
                tsend.at[aligned(me, cap)], back.at[aligned(me, cap)], back_sem.at[zed]
            ).start()

    def backward(step, carry):
        plane = from_plane(step)
        span = aligned(plane, group)
        view = grads.at[core, span]
        local_wait(view, grads_sem.at[plane])
        to_pair(view, PLANES + step).start()

        @pl.when(step > 0)
        def _():
            finish(step - 1)

        to_pair(grads.at[other, span], PLANES + step).wait_recv()
        hidden_grad = dot_nt(grads[0, span, :], wd[:, :half]) + dot_nt(
            grads[1, span, :], wd[:, half:]
        )
        gate = pre[span, :hidden]
        up = pre[span, hidden:]
        sig = jax.nn.sigmoid(gate)
        silu = gate * sig
        hid[span, :] = (silu * up).astype(BF)
        xgu[span, :hidden] = (hidden_grad * up * sig * (1.0 + gate * (1.0 - sig))).astype(BF)
        xgu[span, hidden:] = (hidden_grad * silu).astype(BF)
        psend[span, :] = dot_nt(xgu[span, :], wgu[theirs, :]).astype(BF)
        remote(
            psend.at[span], precv.at[span], pair_send.at[2 * PLANES + step],
            pair_recv.at[2 * PLANES + step], tp=other,
        ).start()
        own[lax.rem(step, 2)] = dot_nt(xgu[span, :], wgu[mine, :])
        return carry

    lax.fori_loop(0, PLANES, backward, 0)
    finish(PLANES - 1)

    tile = 256
    tiles = half // tile

    for side in range(2):
        def weight_tile(step, carry, side=side):
            columns = aligned(step, tile)
            spot = pl.ds(pl.multiple_of(side * half + step * tile, tile), tile)
            dgu[spot, :] = dot_tn(rows[side, :, columns], xgu[...]).astype(BF)
            ddown[:, spot] = dot_tn(hid[...], grads[side, :, columns]).astype(BF)
            return carry

        lax.fori_loop(0, tiles, weight_tile, 0)

    stores = [
        pltpu.make_async_copy(dgu.at[:, pl.ds(0, hidden)], gate_g, load_sem.at[0]),
        pltpu.make_async_copy(dgu.at[:, pl.ds(hidden, hidden)], up_g, load_sem.at[1]),
        pltpu.make_async_copy(ddown, down_g, load_sem.at[2]),
    ]
    for store in stores:
        store.start()

    def gather(step, carry):
        plane = from_plane(step)
        local_wait(back.at[aligned(plane, group)], back_sem.at[plane])
        return carry

    lax.fori_loop(0, PLANES, gather, 0)
    moe = dot_nn(place_t_ref[...], back[...])
    halves[core] = (moe + cot_ref[:, mine].astype(F32)).astype(BF)
    last = to_pair(halves.at[core], 3 * PLANES)
    last.start()
    grad_ref[:, mine] = halves[core]
    to_pair(halves.at[other], 3 * PLANES).wait_recv()
    grad_ref[:, theirs] = halves[other]

    sent_rows = (count - 1) * cap
    for which in range(3):
        local_wait(send_r.at[pl.ds(0, sent_rows)], bulk_sem.at[which])
    shared = plane_ref.at[pl.ds(0, (peers - 1) * tokens)]
    local_wait(shared, bulk_sem.at[3])
    local_wait(shared, mixer_sem.at[0])
    keep.wait()
    for slot in range(2 * PLANES):
        to_pair(rows.at[0, pl.ds(0, group)], slot).wait_send()
    for slot in range(2 * PLANES, 3 * PLANES):
        to_pair(psend.at[pl.ds(0, group)], slot).wait_send()
    last.wait_send()
    for store in stores:
        store.wait()


def expert_exchange(tok, cot, place, place_t, weight, mixer, gate_w, up_w, down_w):
    count = lax.axis_size("sp")
    tokens, width = tok.shape
    slots = place.shape[0]
    cap = slots // count
    half = width // 2
    hidden = gate_w.shape[1]
    peers = count // PLANES
    group = peers * cap
    vmem, anywhere = pl.BlockSpec(memory_space=pltpu.VMEM), pl.BlockSpec(memory_space=pl.ANY)
    dma = pltpu.SemaphoreType.DMA
    flops = 2 * slots * width * hidden * 8
    return pl.pallas_call(
        functools.partial(expert_kernel, count, cap),
        in_specs=[vmem] * 6 + [anywhere] * 3,
        out_specs=[vmem] + [anywhere] * 4,
        out_shape=[
            jax.ShapeDtypeStruct((tokens, width), BF),
            jax.ShapeDtypeStruct((peers * tokens, mixer.shape[1]), BF),
            jax.ShapeDtypeStruct(gate_w.shape, BF),
            jax.ShapeDtypeStruct(up_w.shape, BF),
            jax.ShapeDtypeStruct(down_w.shape, BF),
        ],
        scratch_shapes=[
            pltpu.VMEM((width, 2 * hidden), BF),
            pltpu.VMEM((hidden, width), BF),
            pltpu.VMEM((slots, half), BF),
            pltpu.VMEM((slots, half), BF),
            pltpu.VMEM((2, slots, half), BF),
            pltpu.VMEM((2, slots, half), BF),
            pltpu.VMEM((slots, 2 * hidden), F32),
            pltpu.VMEM((slots, hidden), BF),
            pltpu.VMEM((slots, 2 * hidden), BF),
            pltpu.VMEM((2, group, half), F32),
            pltpu.VMEM((slots, half), BF),
            pltpu.VMEM((slots, half), BF),
            pltpu.VMEM((slots, half), BF),
            pltpu.VMEM((slots, half), BF),
            pltpu.VMEM((2, tokens, half), BF),
            pltpu.VMEM((width, 2 * hidden), BF),
            pltpu.VMEM((hidden, width), BF),
            dma((3,)), dma((4,)), dma((PLANES,)), dma((PLANES,)), dma((PLANES,)), dma((2,)),
            dma((3 * PLANES + 1,)), dma((3 * PLANES + 1,)),
        ],
        compiler_params=pltpu.CompilerParams(
            collective_id=0, has_side_effects=True, vmem_limit_bytes=62 * 1024 * 1024
        ),
        cost_estimate=pl.CostEstimate(flops=flops, bytes_accessed=20 << 20, transcendentals=0),
        name="expert_exchange",
    )(tok, cot, place, place_t, weight, mixer, gate_w, up_w, down_w)


SEGMENTS = 8


def tail_kernel(
    count,
    grad_ref, cols_ref, plane_w, out_w, gelu_ref, slope_ref, decay_ref, first_ref, second_ref,
    third_ref, decay_w, input_w, taps_ref,
    gate_out, recur_out, weight_out,
    outw, mixer, cols, part, send_part, got_part, state, decays, local, cumul, conv_grad, pair, pieces,
    load_sem, bulk_sem, cols_sem, part_sem, carry_send, carry_recv, halo_sem,
):
    me = lax.axis_index("sp")
    peers = count // PLANES
    zed, pos = me // peers, lax.rem(me, peers)
    tokens, channels = gelu_ref.shape
    share = weight_out.shape[0]
    span = tokens // SEGMENTS

    loads = [
        pltpu.make_async_copy(out_w, outw, load_sem.at[0]),
        pltpu.make_async_copy(plane_w, mixer, load_sem.at[1]),
        pltpu.make_async_copy(cols_ref.at[pos], cols.at[aligned(pos, tokens)], load_sem.at[2]),
    ]
    for load in loads:
        load.start()

    barrier = pltpu.get_barrier_semaphore()

    def greet(step, carry):
        pl.semaphore_signal(
            barrier, inc=1, device_id={"sp": lax.rem(me + step, count)}, device_id_type=MESH
        )
        return carry

    lax.fori_loop(1, count, greet, 0)
    pl.semaphore_wait(barrier, count - 1)

    def send_cols(shift, carry):
        place = lax.rem(pos + shift, peers)
        remote(
            cols_ref.at[place], cols.at[aligned(pos, tokens)], bulk_sem.at[0], cols_sem.at[0],
            sp=zed * peers + place,
        ).start()
        return carry

    lax.fori_loop(1, peers, send_cols, 0)

    loads[0].wait()
    mixer_grad = dot_nn(grad_ref[...], outw[...])
    gate_out[...] = (mixer_grad * slope_ref[...]).astype(BF)
    width = decay_w.shape[1]
    blocks = range(channels // width)

    def lanes(block):
        return slice(block * width, (block + 1) * width)

    for block in blocks:
        state[block] = mixer_grad[:, lanes(block)] * gelu_ref[:, lanes(block)]
        decays[block] = decay_ref[:, lanes(block)]

    def scan(step, carry):
        rows = pl.ds(span - 1 - step, SEGMENTS, stride=span)
        after = []
        for block in blocks:
            product, total, decay = carry[block]
            product = product * decay
            total = state[block, rows, :] + decay * total
            cumul[block, rows, :] = product
            local[block, rows, :] = total
            after.append((product, total, decays[block, rows, :]))
        return after

    start = []
    for block in blocks:
        rows = pl.ds(span - 1, SEGMENTS, stride=span)
        decay = decays[block, rows, :]
        total = state[block, rows, :]
        product = decay * 0.0 + 1.0
        cumul[block, rows, :] = product
        local[block, rows, :] = total
        start.append((product, total, decay))
    ended = lax.fori_loop(1, span, scan, start)
    product = jnp.concatenate([ended[block][0] * ended[block][2] for block in blocks], axis=1)
    total = jnp.concatenate([ended[block][1] * ended[block][2] for block in blocks], axis=1)
    whole, entry = product[SEGMENTS - 1 :], total[SEGMENTS - 1 :]
    for segment in range(SEGMENTS - 2, -1, -1):
        row = slice(segment, segment + 1)
        whole = whole * product[row]
        entry = total[row] + product[row] * entry
    pair[0:1, :] = whole
    pair[1:2, :] = entry

    def carry_copy(dest):
        return remote(pair, pieces.at[me], carry_send.at[dest], carry_recv.at[me], sp=dest)

    def send_carry(step, carry):
        carry_copy(me - 1 - step).start()
        return carry

    lax.fori_loop(0, me, send_carry, 0)

    def take_carry(step, entering):
        source = count - 1 - step
        local_wait(pieces.at[source], carry_recv.at[source])
        return pieces[source, 0:1, :] * entering + pieces[source, 1:2, :]

    entering = lax.fori_loop(
        0, count - 1 - me, take_carry, jnp.zeros((1, channels), F32)
    )
    enter = []
    for segment in range(SEGMENTS - 1, -1, -1):
        enter.append(entering)
        row = slice(segment, segment + 1)
        entering = total[row] + product[row] * entering
    enter = jnp.concatenate(enter[::-1], axis=0)

    for block in blocks:
        at = lanes(block)
        spread = jnp.broadcast_to(enter[:, None, at], (SEGMENTS, span, width)).reshape(tokens, width)
        carried = local[block] + cumul[block] * spread
        both = jnp.concatenate(
            [(carried * first_ref[:, at]).astype(BF), (carried * second_ref[:, at]).astype(BF)],
            axis=1,
        )
        maps = jnp.concatenate([decay_w[block], input_w[block]], axis=1)
        conv_grad[0:tokens, at] = carried * third_ref[:, at] + dot_nt(both, maps)

    halo = pl.ds(tokens, 8)

    def halo_copy():
        return remote(
            conv_grad.at[pl.ds(0, 8)], conv_grad.at[halo], halo_sem.at[0], halo_sem.at[1], sp=me - 1
        )

    @pl.when(me > 0)
    def _():
        halo_copy().start()

    @pl.when(me == count - 1)
    def _():
        conv_grad[halo, :] = jnp.zeros((8, channels), F32)

    loads[1].wait()
    loads[2].wait()
    local_wait(cols.at[pl.ds(0, (peers - 1) * tokens)], cols_sem.at[0])
    part[...] = dot_tn(cols[...], mixer[...])
    send_part[...] = part[...].astype(BF)

    def send_block(shift, carry):
        plane = lax.rem(zed + shift, PLANES)
        remote(
            send_part.at[aligned(plane, share)], got_part.at[aligned(zed, share)],
            bulk_sem.at[1], part_sem.at[zed], sp=plane * peers + pos,
        ).start()
        return carry

    lax.fori_loop(1, PLANES, send_block, 0)

    def taps_over(low, high):
        total = taps_ref[0:1, :] * conv_grad[low + 3 : high + 3, :]
        for tap in range(1, 4):
            total = total + taps_ref[tap : tap + 1, :] * conv_grad[low + 3 - tap : high + 3 - tap, :]
        recur_out[low:high, :] = total.astype(BF)

    taps_over(0, tokens - 16)

    @pl.when(me < count - 1)
    def _():
        local_wait(conv_grad.at[halo], halo_sem.at[1])

    taps_over(tokens - 16, tokens)

    summed = part[aligned(zed, share), :]
    for shift in range(1, PLANES):
        plane = lax.rem(zed + shift, PLANES)
        local_wait(got_part.at[aligned(plane, share)], part_sem.at[plane])
        summed = summed + got_part[aligned(plane, share), :].astype(F32)
    weight_out[...] = summed

    local_wait(cols.at[pl.ds(0, (peers - 1) * tokens)], bulk_sem.at[0])
    local_wait(got_part.at[pl.ds(0, (PLANES - 1) * share)], bulk_sem.at[1])

    def sent_carry(step, carry):
        carry_copy(me - 1 - step).wait_send()
        return carry

    lax.fori_loop(0, me, sent_carry, 0)

    @pl.when(me > 0)
    def _():
        halo_copy().wait_send()


def tail_exchange(
    grad, cols, plane, out_weight, gelu, slope, decay, first, second, third, decay_w, input_w, taps
):
    count = lax.axis_size("sp")
    tokens, channels = gelu.shape
    peers = count // PLANES
    total_share = cols.shape[2]
    share = total_share // PLANES
    vmem, anywhere = pl.BlockSpec(memory_space=pltpu.VMEM), pl.BlockSpec(memory_space=pl.ANY)
    dma = pltpu.SemaphoreType.DMA
    flops = 4 * tokens * out_weight.shape[0] * channels
    return pl.pallas_call(
        functools.partial(tail_kernel, count),
        in_specs=[vmem] * 2 + [anywhere] * 2 + [vmem] * 9,
        out_specs=[vmem] * 3,
        out_shape=[
            jax.ShapeDtypeStruct((tokens, channels), BF),
            jax.ShapeDtypeStruct((tokens, channels), BF),
            jax.ShapeDtypeStruct((share, channels), F32),
        ],
        scratch_shapes=[
            pltpu.VMEM(out_weight.shape, BF),
            pltpu.VMEM(plane.shape, BF),
            pltpu.VMEM((peers * tokens, total_share), BF),
            pltpu.VMEM((total_share, channels), F32),
            pltpu.VMEM((total_share, channels), BF),
            pltpu.VMEM((total_share, channels), BF),
            *[pltpu.VMEM((decay_w.shape[0], tokens, decay_w.shape[1]), F32)] * 4,
            pltpu.VMEM((tokens + 8, channels), F32),
            pltpu.VMEM((2, channels), F32),
            pltpu.VMEM((count, 2, channels), F32),
            dma((3,)), dma((2,)), dma((1,)), dma((PLANES,)), dma((count,)), dma((count,)), dma((2,)),
        ],
        compiler_params=pltpu.CompilerParams(
            collective_id=1, has_side_effects=True, vmem_limit_bytes=48 * 1024 * 1024
        ),
        cost_estimate=pl.CostEstimate(flops=flops, bytes_accessed=16 << 20, transcendentals=0),
        name="tail_exchange",
    )(grad, cols, plane, out_weight, gelu, slope, decay, first, second, third, decay_w, input_w, taps)


def passed_along(value, axis, steps):
    count = lax.axis_size(axis)
    initial, last = (max(0, -steps), min(count, count - steps))
    return lax.ppermute(value, axis, [(source, source + steps) for source in range(initial, last)])


def on_device(
    moe_input,
    cotangent,
    expert_ids,
    route_weight,
    gate_proj,
    up_proj,
    down_proj,
    out_weight,
    recur_input,
    gate_input,
    states,
    conv_taps,
    decay_gate_w,
    input_gate_w,
    decay_rate,
    decay_extra,
):
    experts = lax.axis_size("sp")
    tok_rows, width = moe_input.shape
    top_count = expert_ids.shape[1]
    capacity = max(2, 4 * tok_rows // experts)
    slot_count = experts * capacity
    gelu_value, gelu_back = jax.vjp(jax.nn.gelu, gate_input.astype(F32))
    mixer_out = (states * gelu_value).astype(BF)
    slope = states * gelu_back(jnp.ones_like(gelu_value))[0]
    channels = recur_input.shape[1]
    recur_float = recur_input.astype(F32)
    before = passed_along(jnp.concatenate([recur_float[-3:], states[-1:]], axis=0), "sp", 1)
    extended = jnp.concatenate([before[:3], recur_float], axis=0)
    taps = conv_taps.astype(F32)
    conv = taps[0] * extended[0:tok_rows]
    for tap_index in range(1, 4):
        conv = conv + taps[tap_index] * extended[tap_index : tap_index + tok_rows]
    blocks = decay_gate_w.shape[0]
    block_width = decay_gate_w.shape[1]
    conv_blocks = conv.astype(BF).reshape(tok_rows, blocks, block_width)
    decay_pre = jnp.einsum(
        "tbi,bij->tbj", conv_blocks, decay_gate_w, preferred_element_type=F32
    ).reshape(tok_rows, channels)
    input_pre = jnp.einsum(
        "tbi,bij->tbj", conv_blocks, input_gate_w, preferred_element_type=F32
    ).reshape(tok_rows, channels)
    recur_gate = jax.nn.sigmoid(decay_pre)
    input_gate = jax.nn.sigmoid(input_pre)
    positions = lax.axis_index("sp") * tok_rows + jnp.arange(tok_rows, dtype=jnp.int32)
    first_row = (positions == 0)[:, None]
    rate = -decay_scale * decay_rate[None, :]
    log_decay = rate * recur_gate + decay_extra
    decay_value = jnp.exp(log_decay)
    mult = jnp.where(first_row, 1.0, jnp.sqrt(-jnp.expm1(2.0 * log_decay)))
    prev_states = jnp.concatenate([before[3:], states[:-1]], axis=0)
    log_factor = prev_states * decay_value - jnp.where(
        first_row, 0.0, input_gate * conv * decay_value * decay_value / mult
    )
    decay_factor = log_factor * rate * recur_gate * (1.0 - recur_gate)
    input_factor = mult * conv * input_gate * (1.0 - input_gate)
    conv_factor = mult * input_gate

    flat_ids = expert_ids.reshape(-1)
    onehot = (flat_ids[:, None] == jnp.arange(experts, dtype=jnp.int32)[None, :]).astype(jnp.int32)
    slot_rank = jnp.sum((jnp.cumsum(onehot, axis=0) - onehot) * onehot, axis=1)
    pair_slots = (flat_ids * capacity + slot_rank).reshape(tok_rows, top_count)
    slot_iota = jnp.arange(slot_count, dtype=jnp.int32)
    placing = slot_iota[:, None, None] == pair_slots[None, :, :]
    place = jnp.any(placing, axis=2).astype(BF)
    place_t = jnp.any(pair_slots[:, :, None] == slot_iota[None, None, :], axis=1).astype(BF)
    weight = jnp.sum(jnp.where(placing, route_weight[None], 0.0), axis=(1, 2))[:, None]
    input_grad, mixer_plane, gate_weight_grad, up_weight_grad, down_grad = expert_exchange(
        moe_input, cotangent, place, place_t, weight, mixer_out, gate_proj[0], up_proj[0], down_proj[0]
    )
    peers = experts // PLANES
    cols = input_grad.reshape(tok_rows, PLANES, peers, width // experts)
    cols = cols.transpose(2, 0, 1, 3).reshape(peers, tok_rows, width // peers)
    gate_grad, recur_grad, out_weight_grad = tail_exchange(
        input_grad, cols, mixer_plane, out_weight, gelu_value, slope, decay_value,
        decay_factor, input_factor, conv_factor, decay_gate_w, input_gate_w, taps,
    )
    return (
        gate_weight_grad[None],
        up_weight_grad[None],
        down_grad[None],
        out_weight_grad,
        input_grad,
        recur_grad,
        gate_grad,
    )


def solution(mesh):
    return jax.shard_map(
        on_device,
        mesh=mesh,
        in_specs=(
            P("sp", None),
            P("sp", None),
            P("sp", None),
            P("sp", None),
            P("sp", None, "tp"),
            P("sp", None, "tp"),
            P("sp", "tp", None),
            P(None, "tp"),
            P("sp", "tp"),
            P("sp", "tp"),
            P("sp", "tp"),
            P(None, "tp"),
            P("tp", None, None),
            P("tp", None, None),
            P("tp"),
            P("sp", "tp"),
        ),
        out_specs=(
            P("sp", None, "tp"),
            P("sp", None, "tp"),
            P("sp", "tp", None),
            P("sp", "tp"),
            P("sp", None),
            P("sp", "tp"),
            P("sp", "tp"),
        ),
        check_vma=False,
    )
```

```python
import functools

import jax
import jax.numpy as jnp
from jax import lax
from jax.experimental import pallas as pl
from jax.experimental.pallas import tpu as pltpu
from jax.sharding import PartitionSpec as P

decay_scale = 8.0
BF = jnp.bfloat16
F32 = jnp.float32
PLANES = 4
SEGMENTS = 8
LANES = 128
MESH = pl.DeviceIdType.MESH


def dot_nn(left, right):
    return jnp.dot(left, right, preferred_element_type=F32)


def dot_nt(left, right):
    return lax.dot_general(left, right, (((1,), (1,)), ((), ())), preferred_element_type=F32)


def dot_tn(left, right):
    return lax.dot_general(left, right, (((0,), (0,)), ((), ())), preferred_element_type=F32)


def aligned(index, size):
    return pl.ds(pl.multiple_of(index * size, size), size)


def local_wait(view, sem):
    pltpu.make_async_copy(view, view, sem).wait()


def remote(src, dst, send, recv, **where):
    return pltpu.make_async_remote_copy(
        src_ref=src, dst_ref=dst, send_sem=send, recv_sem=recv, device_id=where, device_id_type=MESH
    )


def iota(shape, axis):
    return lax.broadcasted_iota(jnp.int32, shape, axis)


def fallen(rise):
    series = 1.0 - rise * (1.0 / 7.0)
    for order in range(6, 1, -1):
        series = 1.0 - rise * (1.0 / order) * series
    return jnp.where(rise < 0.25, rise * series, 1.0 - jnp.exp(-rise))


def whole_kernel(
    count, cap,
    tok_ref, cot_ref, ids_ref, route_ref, decay_w, input_w, taps_ref, rate_ref,
    gate_w, up_w, down_w, out_w, recur_in, gate_in, states_in, extra_in,
    gate_g, up_g, down_g, weight_out, grad_ref, recur_out, gate_out, plane_ref,
    wgu, wd, place_t, parts, send_r, send_g, rg, pre, hid, xgu, own, psend, precv, back, halves,
    mixer, cols, send_part, got_part, gelu, slope, first, second, third, decays, cumul, local,
    conv_grad, shifted, prev_in, prev_state, pair, pieces, products,
    load_sem, bulk_sem, rows_sem, grads_sem, back_sem, mixer_sem, pair_send, pair_recv,
    before_sem, cols_sem, part_sem, carry_send, carry_recv, halo_sem,
):
    me, core = lax.axis_index("sp"), lax.axis_index("tp")
    other = 1 - core
    peers = count // PLANES
    zed, pos = me // peers, lax.rem(me, peers)
    group = peers * cap
    tokens, width = tok_ref.shape
    slots = count * cap
    half = width // 2
    hidden = wd.shape[0]
    channels = states_in.shape[1]
    blocks = channels // LANES
    segment_rows = tokens // SEGMENTS
    mine, theirs = aligned(core, half), aligned(other, half)
    rows, grads = rg.at[pl.ds(0, 2)], rg.at[pl.ds(2, 2)]

    loads = [
        pltpu.make_async_copy(gate_w, wgu.at[:, pl.ds(0, hidden)], load_sem.at[0]),
        pltpu.make_async_copy(up_w, wgu.at[:, pl.ds(hidden, hidden)], load_sem.at[1]),
        pltpu.make_async_copy(down_w, wd, load_sem.at[2]),
    ]
    inputs = [
        pltpu.make_async_copy(states_in, own.at[0], load_sem.at[3]),
        pltpu.make_async_copy(extra_in, own.at[1], load_sem.at[4]),
        pltpu.make_async_copy(recur_in, psend.at[0], load_sem.at[5]),
        pltpu.make_async_copy(gate_in, psend.at[1], load_sem.at[6]),
    ]
    for load in inputs + loads:
        load.start()

    barrier = pltpu.get_barrier_semaphore()

    def greet(step, carry):
        pl.semaphore_signal(
            barrier, inc=1, device_id={"sp": lax.rem(me + step, count)}, device_id_type=MESH
        )
        return carry

    lax.fori_loop(1, count, greet, 0)
    pl.semaphore_signal(barrier, inc=1, device_id={"tp": other}, device_id_type=MESH)

    ids, route = ids_ref[...], route_ref[...]
    expert = iota((tokens, LANES), 1)
    chosen = [ids[:, k : k + 1] == expert for k in range(2)]
    member = jnp.where(chosen[0] | chosen[1], 1.0, 0.0).astype(BF)
    earlier = (iota((tokens, tokens), 0) > iota((tokens, tokens), 1)).astype(F32).astype(BF)
    rank = dot_nn(earlier, member).astype(BF)
    low = iota((LANES, slots), 0) * cap
    column = iota((LANES, slots), 1)
    widen = jnp.where((column >= low) & (column < low + cap), 1.0, 0.0).astype(BF)
    owner = dot_nn(iota((8, LANES), 1).astype(F32).astype(BF), widen)[0:1]
    place_in = iota((1, slots), 1).astype(F32) - owner * float(cap)
    taken = (dot_nn(member, widen) > 0.5) & (dot_nn(rank, widen) == place_in)
    place_t[...] = jnp.where(taken, 1.0, 0.0).astype(BF)
    scale = jnp.where(chosen[0], route[:, 0:1], 0.0) + jnp.where(chosen[1], route[:, 1:2], 0.0)
    for piece in range(3):
        rounded = scale.astype(BF)
        parts[:, piece * LANES : (piece + 1) * LANES] = rounded
        scale = scale - rounded.astype(F32)

    pl.semaphore_wait(barrier, count)

    keep_rows = 16
    before = [
        remote(
            recur_in.at[pl.ds(tokens - keep_rows, keep_rows)], prev_in,
            before_sem.at[0], before_sem.at[1], sp=me + 1,
        ),
        remote(
            states_in.at[pl.ds(tokens - 8, 8)], prev_state,
            before_sem.at[2], before_sem.at[3], sp=me + 1,
        ),
    ]

    @pl.when(me < count - 1)
    def _():
        for copy in before:
            copy.start()

    def place(step, source, scaled):
        plane = lax.rem(zed + (PLANES - 1 - step), PLANES)
        span = aligned(plane, group)
        chosen_t = place_t[:, span]
        placed = dot_tn(chosen_t, source[:, mine])
        if scaled:
            sums = dot_tn(chosen_t, parts[...])
            sums = sums[:, :LANES] + sums[:, LANES : 2 * LANES] + sums[:, 2 * LANES :]
            slot = iota((group, LANES), 0) + plane * group
            low = iota((group, LANES), 1) * cap
            own_lane = (slot >= low) & (slot < low + cap)
            placed = placed * jnp.sum(jnp.where(own_lane, sums, 0.0), axis=1, keepdims=True)
        return plane, span, placed.astype(BF)

    def spread(step, plane, source, target, which, sem):
        def one(shift, carry):
            dest = plane * peers + lax.rem(pos + shift, peers)
            remote(
                source.at[aligned(dest, cap)], target.at[aligned(me, cap)],
                bulk_sem.at[which], sem, sp=dest,
            ).start()
            return carry

        lax.fori_loop(jnp.where(step == PLANES - 1, 1, 0), peers, one, 0)

        @pl.when(step == PLANES - 1)
        def _():
            pltpu.make_async_copy(
                source.at[aligned(me, cap)], target.at[aligned(me, cap)], sem
            ).start()

    for which, (source, sent, target, sems) in enumerate(
        ((tok_ref, send_r, rows, rows_sem), (cot_ref, send_g, grads, grads_sem))
    ):
        def issue(step, carry, which=which, source=source, sent=sent, target=target, sems=sems):
            plane, span, placed = place(step, source, which == 1)
            sent[span, :] = placed
            spread(step, plane, sent, target.at[core], which, sems.at[zed])
            return carry

        lax.fori_loop(0, PLANES, issue, 0)

    for load in inputs:
        load.wait()

    @pl.when(me > 0)
    def _():
        for copy in before:
            copy.wait_recv()

    @pl.when(me == 0)
    def _():
        prev_in[...] = jnp.zeros_like(prev_in)
        prev_state[...] = jnp.zeros_like(prev_state)

    def recurrence(block, carry):
        at = aligned(block, LANES)
        states = own[0, :, at]
        gate = psend[1, :, at].astype(F32)
        value, back_of = jax.vjp(functools.partial(jax.nn.gelu, approximate=True), gate)
        mixer[:, at] = (states * value).astype(BF)
        gelu[:, at] = value
        slope[:, at] = states * back_of(jnp.ones_like(value))[0]
        shifted[0:8, :] = prev_in[8:16, at].astype(F32)
        shifted[8:, :] = psend[0, :, at].astype(F32)
        conv = taps_ref[0:1, at] * shifted[5 : 5 + tokens, :]
        for tap in range(1, 4):
            conv = conv + taps_ref[tap : tap + 1, at] * shifted[5 + tap : 5 + tap + tokens, :]
        maps = jnp.concatenate([decay_w[block], input_w[block]], axis=1)
        gates = jax.nn.sigmoid(dot_nn(conv.astype(BF), maps))
        recur_gate, input_gate = gates[:, :LANES], gates[:, LANES:]
        rate = -decay_scale * rate_ref[0:1, at]
        log_decay = rate * recur_gate + own[1, :, at]
        decay = jnp.exp(log_decay)
        opening = (iota((tokens, LANES), 0) == 0) & (me == 0)
        mult = jnp.where(opening, 1.0, jnp.sqrt(fallen(-2.0 * log_decay)))
        shifted[0:8, :] = prev_state[:, at]
        shifted[8:, :] = states
        fall = jnp.where(opening, 0.0, input_gate * conv * decay * decay / mult)
        factor = shifted[7 : 7 + tokens, :] * decay - fall
        first[:, at] = factor * rate * recur_gate * (1.0 - recur_gate)
        third_value = mult * input_gate
        second[:, at] = third_value * conv * (1.0 - input_gate)
        third[:, at] = third_value
        decays[block] = decay

        def along(step, carry):
            product, decay = carry
            picked = pl.ds(segment_rows - 1 - step, SEGMENTS, stride=segment_rows)
            product = product * decay
            cumul[block, picked, :] = product
            return product, decays[block, picked, :]

        picked = pl.ds(segment_rows - 1, SEGMENTS, stride=segment_rows)
        decay = decays[block, picked, :]
        product = decay * 0.0 + 1.0
        cumul[block, picked, :] = product
        product, decay = lax.fori_loop(1, segment_rows, along, (product, decay))
        products[:, at] = product * decay
        return carry

    lax.fori_loop(0, blocks, recurrence, 0)

    def share(shift, carry):
        dest = zed * peers + lax.rem(pos + shift, peers)
        remote(
            mixer, plane_ref.at[aligned(pos, tokens)], bulk_sem.at[3], mixer_sem.at[0], sp=dest
        ).start()
        return carry

    lax.fori_loop(1, peers, share, 0)
    keep = pltpu.make_async_copy(mixer, plane_ref.at[aligned(pos, tokens)], mixer_sem.at[1])
    keep.start()

    def from_plane(step):
        return lax.rem(zed + step + 1, PLANES)

    def to_pair(view, slot):
        return remote(view, view, pair_send.at[slot], pair_recv.at[slot], tp=other)

    def pass_rows(step, carry):
        plane = from_plane(step)
        view = rows.at[core, aligned(plane, group)]
        local_wait(view, rows_sem.at[plane])
        to_pair(view, step).start()
        return carry

    lax.fori_loop(0, PLANES, pass_rows, 0)
    for load in loads:
        load.wait()

    def forward(step, carry):
        span = aligned(from_plane(step), group)
        to_pair(rows.at[other, span], step).wait_recv()
        pre[span, :] = dot_nn(rows[0, span, :], wgu[:half, :]) + dot_nn(
            rows[1, span, :], wgu[half:, :]
        )
        return carry

    lax.fori_loop(0, PLANES, forward, 0)
    local_wait(send_r.at[pl.ds(0, (count - 1) * cap)], bulk_sem.at[0])

    def finish(step):
        plane = from_plane(step)
        span = aligned(plane, group)
        to_pair(precv.at[span], 2 * PLANES + step).wait_recv()
        send_r[span, :] = (own[lax.rem(step, 2)] + precv[span, :].astype(F32)).astype(BF)
        spread(step, plane, send_r, back, 2, back_sem.at[zed])

    def swap_part(step, span):
        return remote(
            psend.at[lax.rem(step, 2)], precv.at[span], pair_send.at[2 * PLANES + step],
            pair_recv.at[2 * PLANES + step], tp=other,
        )

    def backward(step, carry):
        plane = from_plane(step)
        span = aligned(plane, group)
        view = grads.at[core, span]
        local_wait(view, grads_sem.at[plane])
        to_pair(view, PLANES + step).start()

        @pl.when(step > 0)
        def _():
            finish(step - 1)

        to_pair(grads.at[other, span], PLANES + step).wait_recv()
        hidden_grad = dot_nt(grads[0, span, :], wd[:, :half]) + dot_nt(
            grads[1, span, :], wd[:, half:]
        )
        gate = pre[span, :hidden]
        up = pre[span, hidden:]
        sig = jax.nn.sigmoid(gate)
        silu = gate * sig
        hid[span, :] = (silu * up).astype(BF)
        xgu[span, :hidden] = (hidden_grad * up * sig * (1.0 + gate * (1.0 - sig))).astype(BF)
        xgu[span, hidden:] = (hidden_grad * silu).astype(BF)

        @pl.when(step > 1)
        def _():
            swap_part(step - 2, span).wait_send()

        psend[lax.rem(step, 2)] = dot_nt(xgu[span, :], wgu[theirs, :]).astype(BF)
        swap_part(step, span).start()
        own[lax.rem(step, 2)] = dot_nt(xgu[span, :], wgu[mine, :])
        return carry

    lax.fori_loop(0, PLANES, backward, 0)
    finish(PLANES - 1)
    out_load = pltpu.make_async_copy(out_w, wgu, load_sem.at[0])
    out_load.start()

    tile = 256

    for side in range(2):
        def weight_tile(step, carry, side=side):
            columns = aligned(step, tile)
            spot = pl.ds(pl.multiple_of(side * half + step * tile, tile), tile)
            both = dot_tn(rows[side, :, columns], xgu[...]).astype(BF)
            gate_g[spot, :] = both[:, :hidden]
            up_g[spot, :] = both[:, hidden:]
            down_g[:, spot] = dot_tn(hid[...], grads[side, :, columns]).astype(BF)
            return carry

        lax.fori_loop(0, half // tile, weight_tile, 0)

    for slot in range(2 * PLANES):
        to_pair(rows.at[0, pl.ds(0, group)], slot).wait_send()
    shared = plane_ref.at[pl.ds(0, (peers - 1) * tokens)]
    local_wait(shared, mixer_sem.at[0])
    keep.wait()
    chunks = peers * tokens // slots
    mixer_loads = [
        pltpu.make_async_copy(
            plane_ref.at[pl.ds(chunk * slots, slots)], rg.at[chunk], load_sem.at[1 + chunk]
        )
        for chunk in range(chunks)
    ]
    for load in mixer_loads:
        load.start()

    def gather(step, carry):
        plane = from_plane(step)
        local_wait(back.at[aligned(plane, group)], back_sem.at[plane])
        return carry

    lax.fori_loop(0, PLANES, gather, 0)
    moe = dot_nn(place_t[...], back[...])
    halves[core] = (moe + cot_ref[:, mine].astype(F32)).astype(BF)
    last = to_pair(halves.at[core], 3 * PLANES)
    last.start()

    cut = width // count
    lane = cols.shape[1] // PLANES
    deep = PLANES // 2

    def column_block(level, place):
        return aligned((level * peers + place) * cut // lane, lane)

    def send_cols(shift, carry):
        place = lax.rem(pos + shift, peers)
        for level in range(deep):
            remote(
                halves.at[core, :, column_block(level, place)],
                cols.at[aligned(pos, tokens), aligned(core * deep + level, lane)],
                bulk_sem.at[4], cols_sem.at[0], sp=zed * peers + place,
            ).start()
        return carry

    lax.fori_loop(1, peers, send_cols, 0)
    kept = [
        pltpu.make_async_copy(
            halves.at[core, :, column_block(level, pos)],
            cols.at[aligned(pos, tokens), aligned(core * deep + level, lane)],
            cols_sem.at[1 + level],
        )
        for level in range(deep)
    ]
    for copy in kept:
        copy.start()

    grad_ref[:, mine] = halves[core]
    out_load.wait()
    to_pair(halves.at[other], 3 * PLANES).wait_recv()
    grad_ref[:, theirs] = halves[other]

    mixer_grad = dot_nn(halves[0], wgu[:half, :]) + dot_nn(halves[1], wgu[half:, :])
    gate_out[...] = (mixer_grad * slope[...]).astype(BF)
    for block in range(blocks):
        at = pl.ds(block * LANES, LANES)
        local[block] = mixer_grad[:, block * LANES : (block + 1) * LANES] * gelu[:, at]

    def scan(step, carry):
        picked = pl.ds(segment_rows - 1 - step, SEGMENTS, stride=segment_rows)
        after = []
        for block in range(blocks):
            total, decay = carry[block]
            total = local[block, picked, :] + decay * total
            local[block, picked, :] = total
            after.append((total, decays[block, picked, :]))
        return after

    picked = pl.ds(segment_rows - 1, SEGMENTS, stride=segment_rows)
    start = [(local[block, picked, :], decays[block, picked, :]) for block in range(blocks)]
    ended = lax.fori_loop(1, segment_rows, scan, start)
    total = jnp.concatenate([piece[0] * piece[1] for piece in ended], axis=1)
    product = products[...]
    whole, entry = product[SEGMENTS - 1 :], total[SEGMENTS - 1 :]
    for segment in range(SEGMENTS - 2, -1, -1):
        row = slice(segment, segment + 1)
        whole = whole * product[row]
        entry = total[row] + product[row] * entry
    pair[0:1, :] = whole
    pair[1:2, :] = entry

    def carry_copy(dest):
        return remote(pair, pieces.at[me], carry_send.at[dest], carry_recv.at[me], sp=dest)

    def send_carry(step, carry):
        carry_copy(me - 1 - step).start()
        return carry

    lax.fori_loop(0, me, send_carry, 0)

    local_wait(cols.at[pl.ds(0, (peers - 1) * tokens), pl.ds(0, deep * lane)], cols_sem.at[0])
    for copy in kept:
        copy.wait()
    cols_mine = cols.at[:, aligned(core, deep * lane)]
    cols_pass = to_pair(cols_mine, 3 * PLANES + 1)
    cols_pass.start()

    def take_carry(step, entering):
        source = count - 1 - step
        local_wait(pieces.at[source], carry_recv.at[source])
        return pieces[source, 0:1, :] * entering + pieces[source, 1:2, :]

    entering = lax.fori_loop(0, count - 1 - me, take_carry, jnp.zeros((1, channels), F32))

    for load in mixer_loads:
        load.wait()
    to_pair(cols.at[:, aligned(other, deep * lane)], 3 * PLANES + 1).wait_recv()
    sums = pl.ds(0, PLANES * lane)
    partial = dot_tn(cols[pl.ds(0, slots), :], rg[0])
    for chunk in range(1, chunks):
        partial = partial + dot_tn(cols[pl.ds(chunk * slots, slots), :], rg[chunk])
    pre[sums, :] = partial
    send_part[...] = partial.astype(BF)

    def part_rows(plane):
        offset = lax.rem((plane * peers + pos) * cut, lane)
        return pl.ds(pl.multiple_of(plane * lane + offset, cut), cut)

    def send_block(shift, carry):
        plane = lax.rem(zed + shift, PLANES)
        remote(
            send_part.at[part_rows(plane)], got_part.at[aligned(zed, cut)],
            bulk_sem.at[5], part_sem.at[zed], sp=plane * peers + pos,
        ).start()
        return carry

    lax.fori_loop(1, PLANES, send_block, 0)

    enter = []
    for segment in range(SEGMENTS - 1, -1, -1):
        enter.append(entering)
        row = slice(segment, segment + 1)
        entering = total[row] + product[row] * entering
    enter = jnp.concatenate(enter[::-1], axis=0)

    for block in range(blocks):
        at = slice(block * LANES, (block + 1) * LANES)
        filled = jnp.broadcast_to(enter[:, None, at], (SEGMENTS, segment_rows, LANES))
        carried = local[block] + cumul[block] * filled.reshape(tokens, LANES)
        both = jnp.concatenate(
            [(carried * first[:, at]).astype(BF), (carried * second[:, at]).astype(BF)], axis=1
        )
        maps = jnp.concatenate([decay_w[block], input_w[block]], axis=1)
        conv_grad[0:tokens, at] = carried * third[:, at] + dot_nt(both, maps)

    halo = pl.ds(tokens, 8)
    halo_copy = remote(
        conv_grad.at[pl.ds(0, 8)], conv_grad.at[halo], halo_sem.at[0], halo_sem.at[1], sp=me - 1
    )

    @pl.when(me > 0)
    def _():
        halo_copy.start()

    @pl.when(me == count - 1)
    def _():
        conv_grad[halo, :] = jnp.zeros((8, channels), F32)

    def taps_over(low, high):
        total = taps_ref[0:1, :] * conv_grad[low + 3 : high + 3, :]
        for tap in range(1, 4):
            total = total + taps_ref[tap : tap + 1, :] * conv_grad[low + 3 - tap : high + 3 - tap, :]
        recur_out[low:high, :] = total.astype(BF)

    taps_over(0, tokens - 16)

    @pl.when(me < count - 1)
    def _():
        local_wait(conv_grad.at[halo], halo_sem.at[1])

    taps_over(tokens - 16, tokens)

    summed = pre[part_rows(zed), :]
    for shift in range(1, PLANES):
        plane = lax.rem(zed + shift, PLANES)
        local_wait(got_part.at[aligned(plane, cut)], part_sem.at[plane])
        summed = summed + got_part[aligned(plane, cut), :].astype(F32)
    weight_out[...] = summed

    local_wait(send_r.at[pl.ds(0, (count - 1) * cap)], bulk_sem.at[1])
    local_wait(send_r.at[pl.ds(0, (count - 1) * cap)], bulk_sem.at[2])
    local_wait(shared, bulk_sem.at[3])
    local_wait(cols.at[pl.ds(0, (peers - 1) * tokens), pl.ds(0, deep * lane)], bulk_sem.at[4])
    local_wait(got_part.at[pl.ds(0, (PLANES - 1) * cut)], bulk_sem.at[5])
    for step in range(PLANES - 2, PLANES):
        swap_part(step, pl.ds(0, group)).wait_send()
    last.wait_send()
    cols_pass.wait_send()

    def sent_carry(step, carry):
        carry_copy(me - 1 - step).wait_send()
        return carry

    lax.fori_loop(0, me, sent_carry, 0)

    @pl.when(me > 0)
    def _():
        halo_copy.wait_send()

    @pl.when(me < count - 1)
    def _():
        for copy in before:
            copy.wait_send()


def flush_kernel(total, *refs):
    sems = refs[-1]
    copies = [
        pltpu.make_async_copy(refs[item], refs[total + item], sems.at[item])
        for item in range(total)
    ]
    for copy in copies:
        copy.start()
    for copy in copies:
        copy.wait()


def flushed(*results):
    total = len(results)
    size = sum(result.size * result.dtype.itemsize for result in results)
    return pl.pallas_call(
        functools.partial(flush_kernel, total),
        in_specs=[pl.BlockSpec(memory_space=pltpu.VMEM)] * total,
        out_specs=[pl.BlockSpec(memory_space=pl.ANY)] * total,
        out_shape=[jax.ShapeDtypeStruct(result.shape, result.dtype) for result in results],
        scratch_shapes=[pltpu.SemaphoreType.DMA((total,))],
        compiler_params=pltpu.CompilerParams(vmem_limit_bytes=4 * 1024 * 1024),
        cost_estimate=pl.CostEstimate(flops=1000, bytes_accessed=2 * size, transcendentals=0),
        name="flush",
    )(*results)


def on_device(
    moe_input,
    cotangent,
    expert_ids,
    route_weight,
    gate_proj,
    up_proj,
    down_proj,
    out_weight,
    recur_input,
    gate_input,
    states,
    conv_taps,
    decay_gate_w,
    input_gate_w,
    decay_rate,
    decay_extra,
):
    count = lax.axis_size("sp")
    tokens, width = moe_input.shape
    cap = max(2, 4 * tokens // count)
    slots = count * cap
    half = width // 2
    hidden = gate_proj.shape[2]
    channels = states.shape[1]
    peers = count // PLANES
    group = peers * cap
    cut = width // count
    lane = max(cut, LANES)
    blocks = channels // LANES
    vmem, anywhere = pl.BlockSpec(memory_space=pltpu.VMEM), pl.BlockSpec(memory_space=pl.ANY)
    dma = pltpu.SemaphoreType.DMA

    def out(shape, kind):
        return jax.ShapeDtypeStruct(shape, kind)

    def plain(kind):
        return pltpu.VMEM((tokens, channels), kind)

    results = pl.pallas_call(
        functools.partial(whole_kernel, count, cap),
        in_specs=[vmem] * 8 + [anywhere] * 8,
        out_specs=[vmem] * 7 + [anywhere],
        out_shape=[
            out((width, hidden), BF), out((width, hidden), BF), out((hidden, width), BF),
            out((cut, channels), F32), out((tokens, width), BF), out((tokens, channels), BF),
            out((tokens, channels), BF), out((peers * tokens, channels), BF),
        ],
        scratch_shapes=[
            pltpu.VMEM((width, 2 * hidden), BF),
            pltpu.VMEM((hidden, width), BF),
            pltpu.VMEM((tokens, slots), BF),
            pltpu.VMEM((tokens, 3 * LANES), BF),
            pltpu.VMEM((slots, half), BF),
            pltpu.VMEM((slots, half), BF),
            pltpu.VMEM((4, slots, half), BF),
            pltpu.VMEM((slots, 2 * hidden), F32),
            pltpu.VMEM((slots, hidden), BF),
            pltpu.VMEM((slots, 2 * hidden), BF),
            pltpu.VMEM((2, group, half), F32),
            pltpu.VMEM((2, group, half), BF),
            pltpu.VMEM((slots, half), BF),
            pltpu.VMEM((slots, half), BF),
            pltpu.VMEM((2, tokens, half), BF),
            plain(BF),
            pltpu.VMEM((peers * tokens, PLANES * lane), BF),
            pltpu.VMEM((PLANES * lane, channels), BF),
            pltpu.VMEM((PLANES * cut, channels), BF),
            plain(F32), plain(F32), plain(F32), plain(F32), plain(F32),
            *[pltpu.VMEM((blocks, tokens, LANES), F32)] * 3,
            pltpu.VMEM((tokens + 8, channels), F32),
            pltpu.VMEM((tokens + 8, LANES), F32),
            pltpu.VMEM((16, channels), BF),
            pltpu.VMEM((8, channels), F32),
            pltpu.VMEM((2, channels), F32),
            pltpu.VMEM((count, 2, channels), F32),
            pltpu.VMEM((SEGMENTS, channels), F32),
            dma((7,)), dma((6,)), dma((PLANES,)), dma((PLANES,)), dma((PLANES,)), dma((2,)),
            dma((3 * PLANES + 2,)), dma((3 * PLANES + 2,)), dma((4,)), dma((3,)), dma((PLANES,)),
            dma((count,)), dma((count,)), dma((2,)),
        ],
        compiler_params=pltpu.CompilerParams(
            collective_id=0, has_side_effects=True, vmem_limit_bytes=62 * 1024 * 1024
        ),
        cost_estimate=pl.CostEstimate(
            flops=16 * slots * width * hidden, bytes_accessed=40 << 20, transcendentals=0
        ),
        name="whole",
    )(
        moe_input, cotangent, expert_ids, route_weight, decay_gate_w, input_gate_w,
        conv_taps.astype(F32), decay_rate[None], gate_proj[0], up_proj[0], down_proj[0], out_weight,
        recur_input, gate_input, states, decay_extra,
    )
    gate_g, up_g, down_g, weight_g, grad, recur_g, gate_in_g = results[:7]
    return (gate_g[None], up_g[None], down_g[None], weight_g, grad, recur_g, gate_in_g)


def solution(mesh):
    return jax.shard_map(
        on_device,
        mesh=mesh,
        in_specs=(
            P("sp", None),
            P("sp", None),
            P("sp", None),
            P("sp", None),
            P("sp", None, "tp"),
            P("sp", None, "tp"),
            P("sp", "tp", None),
            P(None, "tp"),
            P("sp", "tp"),
            P("sp", "tp"),
            P("sp", "tp"),
            P(None, "tp"),
            P("tp", None, None),
            P("tp", None, None),
            P("tp"),
            P("sp", "tp"),
        ),
        out_specs=(
            P("sp", None, "tp"),
            P("sp", None, "tp"),
            P("sp", "tp", None),
            P("sp", "tp"),
            P("sp", None),
            P("sp", "tp"),
            P("sp", "tp"),
        ),
        check_vma=False,
    )
```

```python
import functools

import jax
import jax.numpy as jnp
from jax import lax
from jax.experimental import pallas as pl
from jax.experimental.pallas import tpu as pltpu
from jax.sharding import PartitionSpec as P

decay_scale = 8.0
BF = jnp.bfloat16
F32 = jnp.float32
PLANES = 4
SEGMENTS = 8
LANES = 128
MESH = pl.DeviceIdType.MESH


def dot_nn(left, right):
    return jnp.dot(left, right, preferred_element_type=F32)


def dot_nt(left, right):
    return lax.dot_general(left, right, (((1,), (1,)), ((), ())), preferred_element_type=F32)


def dot_tn(left, right):
    return lax.dot_general(left, right, (((0,), (0,)), ((), ())), preferred_element_type=F32)


def aligned(index, size):
    return pl.ds(pl.multiple_of(index * size, size), size)


def local_wait(view, sem):
    pltpu.make_async_copy(view, view, sem).wait()


def remote(src, dst, send, recv, **where):
    return pltpu.make_async_remote_copy(
        src_ref=src, dst_ref=dst, send_sem=send, recv_sem=recv, device_id=where, device_id_type=MESH
    )


def iota(shape, axis):
    return lax.broadcasted_iota(jnp.int32, shape, axis)


def fallen(rise):
    series = 1.0 - rise * (1.0 / 7.0)
    for order in range(6, 1, -1):
        series = 1.0 - rise * (1.0 / order) * series
    return jnp.where(rise < 0.25, rise * series, 1.0 - jnp.exp(-rise))


def whole_kernel(
    count, cap,
    tok_ref, cot_ref, ids_ref, route_ref, decay_w, input_w, taps_ref, rate_ref,
    gate_w, up_w, down_w, out_w, recur_in, gate_in, states_in, extra_in,
    gate_g, up_g, down_g, weight_out, grad_ref, recur_out, gate_out, plane_ref,
    wgu, wd, table, slot_scale, near_tok, near_cot, far_tok, far_cot, far_ids, far_route, far_moe,
    send_r, send_g, rg, pre, hid, xgu, own, psend, precv, back, halves,
    cols, send_part, got_part, gelu, slope, first, second, third, decays, cumul, local,
    edge, shifted, prev_in, prev_state, pieces, plane_pair, plane_pieces, products,
    load_sem, bulk_sem, rows_sem, grads_sem, back_sem, mixer_sem, pair_send, pair_recv,
    before_sem, cols_sem, part_sem, carry_recv, plane_send, plane_recv, halo_sem, far_send, far_recv,
):
    me, core = lax.axis_index("sp"), lax.axis_index("tp")
    other = 1 - core
    peers = count // PLANES
    zed, pos = me // peers, lax.rem(me, peers)
    group = peers * cap
    tokens, width = tok_ref.shape
    slots = count * cap
    half = width // 2
    hidden = wd.shape[0]
    channels = states_in.shape[1]
    blocks = channels // LANES
    segment_rows = tokens // SEGMENTS
    mine, theirs = aligned(core, half), aligned(other, half)
    deep = PLANES // 2
    base = zed // deep * deep
    far = lax.rem(zed + deep, PLANES) * peers + pos
    near_slots = slots // 2
    conv_grad = own.at[0]
    mixer = send_part.at[pl.ds(0, tokens)]
    rows, grads = rg.at[pl.ds(0, 2)], rg.at[pl.ds(2, 2)]

    loads = [
        pltpu.make_async_copy(gate_w, wgu.at[:, pl.ds(0, hidden)], load_sem.at[0]),
        pltpu.make_async_copy(up_w, wgu.at[:, pl.ds(hidden, hidden)], load_sem.at[1]),
        pltpu.make_async_copy(down_w, wd, load_sem.at[2]),
    ]
    inputs = [
        pltpu.make_async_copy(states_in, own.at[0], load_sem.at[3]),
        pltpu.make_async_copy(extra_in, own.at[1], load_sem.at[4]),
        pltpu.make_async_copy(recur_in, psend.at[0], load_sem.at[5]),
        pltpu.make_async_copy(gate_in, psend.at[1], load_sem.at[6]),
    ]
    near_loads = [
        pltpu.make_async_copy(tok_ref.at[:, mine], near_tok, load_sem.at[7]),
        pltpu.make_async_copy(cot_ref.at[:, mine], near_cot, load_sem.at[8]),
    ]
    for load in near_loads + inputs + loads:
        load.start()

    barrier = pltpu.get_barrier_semaphore()

    def greet(step, carry):
        pl.semaphore_signal(
            barrier, inc=1, device_id={"sp": lax.rem(me + step, count)}, device_id_type=MESH
        )
        return carry

    lax.fori_loop(1, count, greet, 0)
    pl.semaphore_signal(barrier, inc=1, device_id={"tp": other}, device_id_type=MESH)

    def tabulate(kind, ids, route):
        expert = iota((LANES, tokens), 0) + base * peers
        chosen = [ids[k : k + 1, :] == expert for k in range(2)]
        inside = iota((LANES, tokens), 0) < deep * peers
        member = jnp.where((chosen[0] | chosen[1]) & inside, 1.0, 0.0).astype(BF)
        earlier = (iota((tokens, tokens), 0) < iota((tokens, tokens), 1)).astype(F32).astype(BF)
        rank = dot_nn(member, earlier).astype(BF)
        low = iota((near_slots, LANES), 1) * cap
        row = iota((near_slots, LANES), 0)
        within = (row >= low) & (row < low + cap)
        widen = jnp.where(within, 1.0, 0.0).astype(BF)
        place_in = jnp.sum(jnp.where(within, (row - low).astype(F32), 0.0), axis=1, keepdims=True)
        taken = (dot_nn(widen, member) > 0.5) & (dot_nn(widen, rank) == place_in)
        table[kind] = jnp.where(taken, 1.0, 0.0).astype(BF)
        scale = jnp.where(chosen[0], route[0:1, :], 0.0) + jnp.where(chosen[1], route[1:2, :], 0.0)
        total = jnp.zeros((near_slots, tokens), F32)
        for _ in range(3):
            rounded = scale.astype(BF)
            total = total + dot_nn(widen, rounded)
            scale = scale - rounded.astype(F32)
        slot_scale[kind] = jnp.sum(jnp.where(taken, total, 0.0), axis=1, keepdims=True)

    tabulate(0, ids_ref[...], route_ref[...])
    pl.semaphore_wait(barrier, count)

    keep_rows = 16
    before = [
        remote(
            recur_in.at[pl.ds(tokens - keep_rows, keep_rows)], prev_in,
            before_sem.at[0], before_sem.at[1], sp=me + 1,
        ),
        remote(
            states_in.at[pl.ds(tokens - 8, 8)], prev_state,
            before_sem.at[2], before_sem.at[3], sp=me + 1,
        ),
    ]

    @pl.when(me < count - 1)
    def _():
        for copy in before:
            copy.start()

    to_far = [
        remote(ids_ref, far_ids, far_send.at[0], far_recv.at[0], sp=far),
        remote(route_ref, far_route, far_send.at[1], far_recv.at[1], sp=far),
        remote(tok_ref.at[:, mine], far_tok, far_send.at[2], far_recv.at[2], sp=far),
        remote(cot_ref.at[:, mine], far_cot, far_send.at[3], far_recv.at[3], sp=far),
    ]
    for copy in to_far:
        copy.start()

    def spread(level, source, target, which, sem):
        plane = base + level

        def one(shift, carry):
            spot = lax.rem(pos + shift, peers)
            remote(
                source(plane * peers + spot), target, bulk_sem.at[which], sem,
                sp=plane * peers + spot,
            ).start()
            return carry

        here = plane == zed
        lax.fori_loop(jnp.where(here, 1, 0), peers, one, 0)

        @pl.when(here)
        def _():
            pltpu.make_async_copy(source(me), target, sem).start()

    def dispatch(kind, which):
        tokens_in = (
            (near_tok, near_cot) if kind == 0 else (far_tok, far_cot)
        )[which]
        sent = (send_r, send_g)[which]
        target = (rows, grads)[which]
        sems = (rows_sem, grads_sem)[which]
        origin = me if kind == 0 else far
        plane_of = zed if kind == 0 else lax.rem(zed + deep, PLANES)

        def issue(step, carry):
            level = lax.rem(zed - base + 1 + step, deep)
            span = aligned(level, group)
            placed = dot_nn(table[kind, span, :], tokens_in[...])
            if which == 1:
                placed = placed * slot_scale[kind, span, :]
            sent[kind, span, :] = placed.astype(BF)
            spread(
                level,
                lambda dest: sent.at[kind, aligned(dest - base * peers, cap)],
                target.at[core, aligned(origin, cap)], which, sems.at[plane_of],
            )
            return carry

        lax.fori_loop(0, deep, issue, 0)

    near_loads[0].wait()
    dispatch(0, 0)
    near_loads[1].wait()
    dispatch(0, 1)

    for load in inputs:
        load.wait()

    @pl.when(me > 0)
    def _():
        for copy in before:
            copy.wait_recv()

    @pl.when(me == 0)
    def _():
        prev_in[...] = jnp.zeros_like(prev_in)
        prev_state[...] = jnp.zeros_like(prev_state)

    def recurrence(block, carry):
        at = aligned(block, LANES)
        states = own[0, :, at]
        gate = psend[1, :, at].astype(F32)
        value, back_of = jax.vjp(functools.partial(jax.nn.gelu, approximate=True), gate)
        mixer[:, at] = (states * value).astype(BF)
        gelu[:, at] = value
        slope[:, at] = states * back_of(jnp.ones_like(value))[0]
        shifted[0:8, :] = prev_in[8:16, at].astype(F32)
        shifted[8:, :] = psend[0, :, at].astype(F32)
        conv = taps_ref[0:1, at] * shifted[5 : 5 + tokens, :]
        for tap in range(1, 4):
            conv = conv + taps_ref[tap : tap + 1, at] * shifted[5 + tap : 5 + tap + tokens, :]
        maps = jnp.concatenate([decay_w[block], input_w[block]], axis=1)
        gates = jax.nn.sigmoid(dot_nn(conv.astype(BF), maps))
        recur_gate, input_gate = gates[:, :LANES], gates[:, LANES:]
        rate = -decay_scale * rate_ref[0:1, at]
        log_decay = rate * recur_gate + own[1, :, at]
        decay = jnp.exp(log_decay)
        opening = (iota((tokens, LANES), 0) == 0) & (me == 0)
        mult = jnp.where(opening, 1.0, jnp.sqrt(fallen(-2.0 * log_decay)))
        shifted[0:8, :] = prev_state[:, at]
        shifted[8:, :] = states
        fall = jnp.where(opening, 0.0, input_gate * conv * decay * decay / mult)
        factor = shifted[7 : 7 + tokens, :] * decay - fall
        first[:, at] = factor * rate * recur_gate * (1.0 - recur_gate)
        third_value = mult * input_gate
        second[:, at] = third_value * conv * (1.0 - input_gate)
        third[:, at] = third_value
        decays[block] = decay

        def along(step, carry):
            product, decay = carry
            picked = pl.ds(segment_rows - 1 - step, SEGMENTS, stride=segment_rows)
            product = product * decay
            cumul[block, picked, :] = product
            return product, decays[block, picked, :]

        picked = pl.ds(segment_rows - 1, SEGMENTS, stride=segment_rows)
        decay = decays[block, picked, :]
        product = decay * 0.0 + 1.0
        cumul[block, picked, :] = product
        product, decay = lax.fori_loop(1, segment_rows, along, (product, decay))
        products[:, at] = product * decay
        return carry

    lax.fori_loop(0, blocks, recurrence, 0)

    def share(shift, carry):
        dest = zed * peers + lax.rem(pos + shift, peers)
        remote(
            mixer, plane_ref.at[aligned(pos, tokens)], bulk_sem.at[3], mixer_sem.at[0], sp=dest
        ).start()
        return carry

    lax.fori_loop(1, peers, share, 0)
    keep = pltpu.make_async_copy(mixer, plane_ref.at[aligned(pos, tokens)], mixer_sem.at[1])
    keep.start()

    to_far[0].wait_recv()
    to_far[1].wait_recv()
    tabulate(1, far_ids[...], far_route[...])
    to_far[2].wait_recv()
    dispatch(1, 0)

    def from_plane(step):
        return lax.rem(base + deep * (step // deep) + lax.rem(zed - base + step, deep), PLANES)

    def to_pair(view, slot):
        return remote(view, view, pair_send.at[slot], pair_recv.at[slot], tp=other)

    def pass_rows(step, carry):
        plane = from_plane(step)
        view = rows.at[core, aligned(plane, group)]
        local_wait(view, rows_sem.at[plane])
        to_pair(view, step).start()
        return carry

    lax.fori_loop(0, deep, pass_rows, 0)
    for load in loads:
        load.wait()

    def forward(step, carry):
        span = aligned(from_plane(step), group)
        to_pair(rows.at[other, span], step).wait_recv()
        pre[span, :] = dot_nn(rows[0, span, :], wgu[:half, :]) + dot_nn(
            rows[1, span, :], wgu[half:, :]
        )
        return carry

    lax.fori_loop(0, deep, forward, 0)
    to_far[3].wait_recv()
    dispatch(1, 1)
    lax.fori_loop(deep, PLANES, pass_rows, 0)
    lax.fori_loop(deep, PLANES, forward, 0)
    sent_bytes = precv.at[pl.ds(0, 2 * (deep * peers - 1) * cap)]
    local_wait(sent_bytes, bulk_sem.at[0])

    def finish(step):
        plane = from_plane(step)
        span = aligned(plane, group)
        to_pair(precv.at[span], 2 * PLANES + step).wait_recv()
        kind = step // deep
        level = lax.rem(plane, deep)
        near = aligned(level, group)
        send_r[kind, near, :] = (own[lax.rem(step, 2)] + precv[span, :].astype(F32)).astype(BF)
        spread(
            level,
            lambda dest: send_r.at[kind, aligned(dest - base * peers, cap)],
            back.at[kind, aligned(me - base * peers, cap)], 2, back_sem.at[kind * deep + zed - base],
        )

    def swap_part(step, span):
        return remote(
            psend.at[lax.rem(step, 2)], precv.at[span], pair_send.at[2 * PLANES + step],
            pair_recv.at[2 * PLANES + step], tp=other,
        )

    def backward(step, carry):
        plane = from_plane(step)
        span = aligned(plane, group)
        view = grads.at[core, span]
        local_wait(view, grads_sem.at[plane])
        to_pair(view, PLANES + step).start()

        @pl.when(step > 0)
        def _():
            finish(step - 1)

        to_pair(grads.at[other, span], PLANES + step).wait_recv()
        hidden_grad = dot_nt(grads[0, span, :], wd[:, :half]) + dot_nt(
            grads[1, span, :], wd[:, half:]
        )
        gate = pre[span, :hidden]
        up = pre[span, hidden:]
        sig = jax.nn.sigmoid(gate)
        silu = gate * sig
        hid[span, :] = (silu * up).astype(BF)
        xgu[span, :hidden] = (hidden_grad * up * sig * (1.0 + gate * (1.0 - sig))).astype(BF)
        xgu[span, hidden:] = (hidden_grad * silu).astype(BF)

        @pl.when(step > 1)
        def _():
            swap_part(step - 2, span).wait_send()

        psend[lax.rem(step, 2)] = dot_nt(xgu[span, :], wgu[theirs, :]).astype(BF)
        swap_part(step, span).start()
        own[lax.rem(step, 2)] = dot_nt(xgu[span, :], wgu[mine, :])
        return carry

    lax.fori_loop(0, PLANES, backward, 0)
    finish(PLANES - 1)
    out_load = pltpu.make_async_copy(out_w, wgu, load_sem.at[0])
    out_load.start()

    tile = 256

    def weigh(side):
        def weight_tile(step, carry):
            columns = aligned(step, tile)
            spot = pl.ds(pl.multiple_of(side * half + step * tile, tile), tile)
            both = dot_tn(rows[side, :, columns], xgu[...]).astype(BF)
            gate_g[spot, :] = both[:, :hidden]
            up_g[spot, :] = both[:, hidden:]
            down_g[:, spot] = dot_tn(hid[...], grads[side, :, columns]).astype(BF)
            return carry

        lax.fori_loop(0, half // tile, weight_tile, 0)

    weigh(0)

    def gather(step, carry):
        kind, level = step // deep, lax.rem(step, deep)
        local_wait(back.at[kind, aligned(level, group)], back_sem.at[step])
        return carry

    lax.fori_loop(deep, PLANES, gather, 0)
    far_tok[...] = dot_tn(table[1], back[1]).astype(BF)
    far_sum = remote(far_tok, far_moe, far_send.at[4], far_recv.at[4], sp=far)
    far_sum.start()
    weigh(1)
    for slot in range(2 * PLANES):
        to_pair(rows.at[0, pl.ds(0, group)], slot).wait_send()
    shared = plane_ref.at[pl.ds(0, (peers - 1) * tokens)]
    local_wait(shared, mixer_sem.at[0])
    keep.wait()
    local_wait(shared, bulk_sem.at[3])
    chunks = peers * tokens // slots
    mixer_loads = [
        pltpu.make_async_copy(
            plane_ref.at[pl.ds(chunk * slots, slots)], rg.at[chunk], load_sem.at[1 + chunk]
        )
        for chunk in range(chunks)
    ]
    for load in mixer_loads:
        load.start()

    lax.fori_loop(0, deep, gather, 0)
    moe = dot_tn(table[0], back[0]) + near_cot[...].astype(F32)
    far_sum.wait_recv()
    halves[core] = (moe + far_moe[...].astype(F32)).astype(BF)
    last = to_pair(halves.at[core], 3 * PLANES)
    last.start()

    cut = width // count
    lane = cols.shape[1] // PLANES

    def column_block(level, place):
        return aligned((level * peers + place) * cut // lane, lane)

    def send_cols(shift, carry):
        place = lax.rem(pos + shift, peers)
        for level in range(deep):
            remote(
                halves.at[core, :, column_block(level, place)],
                cols.at[aligned(pos, tokens), aligned(core * deep + level, lane)],
                bulk_sem.at[4], cols_sem.at[0], sp=zed * peers + place,
            ).start()
        return carry

    lax.fori_loop(1, peers, send_cols, 0)
    kept = [
        pltpu.make_async_copy(
            halves.at[core, :, column_block(level, pos)],
            cols.at[aligned(pos, tokens), aligned(core * deep + level, lane)],
            cols_sem.at[1 + level],
        )
        for level in range(deep)
    ]
    for copy in kept:
        copy.start()

    grad_ref[:, mine] = halves[core]
    out_load.wait()
    to_pair(halves.at[other], 3 * PLANES).wait_recv()
    grad_ref[:, theirs] = halves[other]

    mixer_grad = dot_nn(halves[0], wgu[:half, :]) + dot_nn(halves[1], wgu[half:, :])
    gate_out[...] = (mixer_grad * slope[...]).astype(BF)
    for block in range(blocks):
        at = pl.ds(block * LANES, LANES)
        local[block] = mixer_grad[:, block * LANES : (block + 1) * LANES] * gelu[:, at]

    def scan(step, carry):
        picked = pl.ds(segment_rows - 1 - step, SEGMENTS, stride=segment_rows)
        after = []
        for block in range(blocks):
            total, decay = carry[block]
            total = local[block, picked, :] + decay * total
            local[block, picked, :] = total
            after.append((total, decays[block, picked, :]))
        return after

    picked = pl.ds(segment_rows - 1, SEGMENTS, stride=segment_rows)
    start = [(local[block, picked, :], decays[block, picked, :]) for block in range(blocks)]
    ended = lax.fori_loop(1, segment_rows, scan, start)
    total = jnp.concatenate([piece[0] * piece[1] for piece in ended], axis=1)
    product = products[...]
    whole, entry = product[SEGMENTS - 1 :], total[SEGMENTS - 1 :]
    for segment in range(SEGMENTS - 2, -1, -1):
        row = slice(segment, segment + 1)
        whole = whole * product[row]
        entry = total[row] + product[row] * entry
    pieces[pos, 0:1, :] = whole
    pieces[pos, 1:2, :] = entry

    def send_carry(shift, carry):
        dest = zed * peers + lax.rem(pos + shift, peers)
        remote(pieces.at[pos], pieces.at[pos], bulk_sem.at[6], carry_recv.at[pos], sp=dest).start()
        return carry

    lax.fori_loop(1, peers, send_carry, 0)

    def wait_carry(shift, carry):
        source = lax.rem(pos + shift, peers)
        local_wait(pieces.at[source], carry_recv.at[source])
        return carry

    lax.fori_loop(1, peers, wait_carry, 0)
    blank = whole * 0.0
    whole, entry = blank + 1.0, blank
    after, after_entry = whole, entry
    for spot in range(peers - 1, -1, -1):
        factor, addend = pieces[spot, 0:1, :], pieces[spot, 1:2, :]
        whole = factor * whole
        entry = addend + factor * entry
        later = spot > pos
        after = jnp.where(later, factor * after, after)
        after_entry = jnp.where(later, addend + factor * after_entry, after_entry)
    plane_pair[0:1, :] = whole
    plane_pair[1:2, :] = entry

    def plane_copy(plane):
        return remote(
            plane_pair, plane_pieces.at[zed], plane_send.at[plane], plane_recv.at[zed],
            sp=plane * peers + pos,
        )

    def send_plane(step, carry):
        plane_copy(zed - 1 - step).start()
        return carry

    lax.fori_loop(0, zed, send_plane, 0)

    local_wait(cols.at[pl.ds(0, (peers - 1) * tokens), pl.ds(0, deep * lane)], cols_sem.at[0])
    for copy in kept:
        copy.wait()
    cols_mine = cols.at[:, aligned(core, deep * lane)]
    cols_pass = to_pair(cols_mine, 3 * PLANES + 1)
    cols_pass.start()

    for load in mixer_loads:
        load.wait()
    to_pair(cols.at[:, aligned(other, deep * lane)], 3 * PLANES + 1).wait_recv()
    sums = pl.ds(0, PLANES * lane)
    partial = dot_tn(cols[pl.ds(0, slots), :], rg[0])
    for chunk in range(1, chunks):
        partial = partial + dot_tn(cols[pl.ds(chunk * slots, slots), :], rg[chunk])
    pre[sums, :] = partial
    send_part[...] = partial.astype(BF)

    def part_rows(plane):
        offset = lax.rem((plane * peers + pos) * cut, lane)
        return pl.ds(pl.multiple_of(plane * lane + offset, cut), cut)

    def send_block(shift, carry):
        plane = lax.rem(zed + shift, PLANES)
        remote(
            send_part.at[part_rows(plane)], got_part.at[aligned(zed, cut)],
            bulk_sem.at[5], part_sem.at[zed], sp=plane * peers + pos,
        ).start()
        return carry

    lax.fori_loop(1, PLANES, send_block, 0)

    def take_plane(step, entering):
        source = PLANES - 1 - step
        local_wait(plane_pieces.at[source], plane_recv.at[source])
        return plane_pieces[source, 0:1, :] * entering + plane_pieces[source, 1:2, :]

    entering = lax.fori_loop(0, PLANES - 1 - zed, take_plane, blank)
    entering = after_entry + after * entering
    enter = []
    for segment in range(SEGMENTS - 1, -1, -1):
        enter.append(entering)
        row = slice(segment, segment + 1)
        entering = total[row] + product[row] * entering
    enter = jnp.concatenate(enter[::-1], axis=0)

    for block in range(blocks):
        at = slice(block * LANES, (block + 1) * LANES)
        filled = jnp.broadcast_to(enter[:, None, at], (SEGMENTS, segment_rows, LANES))
        carried = local[block] + cumul[block] * filled.reshape(tokens, LANES)
        both = jnp.concatenate(
            [(carried * first[:, at]).astype(BF), (carried * second[:, at]).astype(BF)], axis=1
        )
        maps = jnp.concatenate([decay_w[block], input_w[block]], axis=1)
        conv_grad[0:tokens, at] = carried * third[:, at] + dot_nt(both, maps)

    halo = pl.ds(16, 8)
    halo_copy = remote(
        conv_grad.at[pl.ds(0, 8)], edge.at[halo], halo_sem.at[0], halo_sem.at[1], sp=me - 1
    )

    @pl.when(me > 0)
    def _():
        halo_copy.start()

    @pl.when(me == count - 1)
    def _():
        edge[halo, :] = jnp.zeros((8, channels), F32)

    edge[0:16, :] = conv_grad[tokens - 16 : tokens, :]

    def taps_over(source, rows):
        total = taps_ref[0:1, :] * source[3 : rows + 3, :]
        for tap in range(1, 4):
            total = total + taps_ref[tap : tap + 1, :] * source[3 - tap : rows + 3 - tap, :]
        return total.astype(BF)

    recur_out[0 : tokens - 16, :] = taps_over(conv_grad, tokens - 16)

    @pl.when(me < count - 1)
    def _():
        local_wait(edge.at[halo], halo_sem.at[1])

    recur_out[tokens - 16 : tokens, :] = taps_over(edge, 16)

    summed = pre[part_rows(zed), :]
    for shift in range(1, PLANES):
        plane = lax.rem(zed + shift, PLANES)
        local_wait(got_part.at[aligned(plane, cut)], part_sem.at[plane])
        summed = summed + got_part[aligned(plane, cut), :].astype(F32)
    weight_out[...] = summed

    for which in (1, 2):
        local_wait(sent_bytes, bulk_sem.at[which])
    local_wait(pieces.at[pl.ds(0, peers - 1)], bulk_sem.at[6])
    for copy in to_far:
        copy.wait_send()
    far_sum.wait_send()
    local_wait(cols.at[pl.ds(0, (peers - 1) * tokens), pl.ds(0, deep * lane)], bulk_sem.at[4])
    local_wait(got_part.at[pl.ds(0, (PLANES - 1) * cut)], bulk_sem.at[5])
    for step in range(PLANES - 2, PLANES):
        swap_part(step, pl.ds(0, group)).wait_send()
    last.wait_send()
    cols_pass.wait_send()

    def sent_plane(step, carry):
        plane_copy(zed - 1 - step).wait_send()
        return carry

    lax.fori_loop(0, zed, sent_plane, 0)

    @pl.when(me > 0)
    def _():
        halo_copy.wait_send()

    @pl.when(me < count - 1)
    def _():
        for copy in before:
            copy.wait_send()


def flush_kernel(total, *refs):
    sems = refs[-1]
    copies = [
        pltpu.make_async_copy(refs[item], refs[total + item], sems.at[item])
        for item in range(total)
    ]
    for copy in copies:
        copy.start()
    for copy in copies:
        copy.wait()


def flushed(*results):
    total = len(results)
    size = sum(result.size * result.dtype.itemsize for result in results)
    return pl.pallas_call(
        functools.partial(flush_kernel, total),
        in_specs=[pl.BlockSpec(memory_space=pltpu.VMEM)] * total,
        out_specs=[pl.BlockSpec(memory_space=pl.ANY)] * total,
        out_shape=[jax.ShapeDtypeStruct(result.shape, result.dtype) for result in results],
        scratch_shapes=[pltpu.SemaphoreType.DMA((total,))],
        compiler_params=pltpu.CompilerParams(vmem_limit_bytes=4 * 1024 * 1024),
        cost_estimate=pl.CostEstimate(flops=1000, bytes_accessed=2 * size, transcendentals=0),
        name="flush",
    )(*results)


def on_device(
    moe_input,
    cotangent,
    expert_ids,
    route_weight,
    gate_proj,
    up_proj,
    down_proj,
    out_weight,
    recur_input,
    gate_input,
    states,
    conv_taps,
    decay_gate_w,
    input_gate_w,
    decay_rate,
    decay_extra,
):
    count = lax.axis_size("sp")
    tokens, width = moe_input.shape
    cap = max(2, 4 * tokens // count)
    slots = count * cap
    half = width // 2
    hidden = gate_proj.shape[2]
    channels = states.shape[1]
    peers = count // PLANES
    group = peers * cap
    cut = width // count
    lane = max(cut, LANES)
    blocks = channels // LANES
    vmem, anywhere = pl.BlockSpec(memory_space=pltpu.VMEM), pl.BlockSpec(memory_space=pl.ANY)
    dma = pltpu.SemaphoreType.DMA

    def out(shape, kind):
        return pltpu.VMEM(shape, kind)

    def plain(kind):
        return pltpu.VMEM((tokens, channels), kind)

    results = pl.pallas_call(
        functools.partial(whole_kernel, count, cap),
        in_specs=[anywhere] * 2 + [vmem] * 6 + [anywhere] * 8,
        out_specs=[vmem] * 7 + [anywhere],
        out_shape=[
            out((width, hidden), BF), out((width, hidden), BF), out((hidden, width), BF),
            out((cut, channels), F32), out((tokens, width), BF), out((tokens, channels), BF),
            out((tokens, channels), BF), jax.ShapeDtypeStruct((peers * tokens, channels), BF),
        ],
        scratch_shapes=[
            pltpu.VMEM((width, 2 * hidden), BF),
            pltpu.VMEM((hidden, width), BF),
            pltpu.VMEM((2, slots // 2, tokens), BF),
            pltpu.VMEM((2, slots // 2, 1), F32),
            pltpu.VMEM((tokens, half), BF),
            pltpu.VMEM((tokens, half), BF),
            pltpu.VMEM((tokens, half), BF),
            pltpu.VMEM((tokens, half), BF),
            pltpu.VMEM((2, tokens), jnp.int32),
            pltpu.VMEM((2, tokens), F32),
            pltpu.VMEM((tokens, half), BF),
            pltpu.VMEM((2, slots // 2, half), BF),
            pltpu.VMEM((2, slots // 2, half), BF),
            pltpu.VMEM((4, slots, half), BF),
            pltpu.VMEM((slots, 2 * hidden), F32),
            pltpu.VMEM((slots, hidden), BF),
            pltpu.VMEM((slots, 2 * hidden), BF),
            pltpu.VMEM((2, group, half), F32),
            pltpu.VMEM((2, group, half), BF),
            pltpu.VMEM((slots, half), BF),
            pltpu.VMEM((2, slots // 2, half), BF),
            pltpu.VMEM((2, tokens, half), BF),
            pltpu.VMEM((peers * tokens, PLANES * lane), BF),
            pltpu.VMEM((PLANES * lane, channels), BF),
            pltpu.VMEM((PLANES * cut, channels), BF),
            plain(F32), plain(F32), plain(F32), plain(F32), plain(F32),
            *[pltpu.VMEM((blocks, tokens, LANES), F32)] * 3,
            pltpu.VMEM((24, channels), F32),
            pltpu.VMEM((tokens + 8, LANES), F32),
            pltpu.VMEM((16, channels), BF),
            pltpu.VMEM((8, channels), F32),
            pltpu.VMEM((peers, 2, channels), F32),
            pltpu.VMEM((2, channels), F32),
            pltpu.VMEM((PLANES, 2, channels), F32),
            pltpu.VMEM((SEGMENTS, channels), F32),
            dma((9,)), dma((7,)), dma((PLANES,)), dma((PLANES,)), dma((PLANES,)), dma((2,)),
            dma((3 * PLANES + 2,)), dma((3 * PLANES + 2,)), dma((4,)), dma((3,)), dma((PLANES,)),
            dma((peers,)), dma((PLANES,)), dma((PLANES,)), dma((2,)), dma((5,)), dma((5,)),
        ],
        compiler_params=pltpu.CompilerParams(
            collective_id=0, has_side_effects=True, vmem_limit_bytes=54 * 1024 * 1024
        ),
        cost_estimate=pl.CostEstimate(
            flops=16 * slots * width * hidden, bytes_accessed=40 << 20, transcendentals=0
        ),
        name="whole",
    )(
        moe_input, cotangent, expert_ids.T, route_weight.T, decay_gate_w, input_gate_w,
        conv_taps.astype(F32), decay_rate[None], gate_proj[0], up_proj[0], down_proj[0], out_weight,
        recur_input, gate_input, states, decay_extra,
    )
    gate_g, up_g, down_g, weight_g, grad, recur_g, gate_in_g = flushed(*results[:7])
    return (gate_g[None], up_g[None], down_g[None], weight_g, grad, recur_g, gate_in_g)


def solution(mesh):
    return jax.shard_map(
        on_device,
        mesh=mesh,
        in_specs=(
            P("sp", None),
            P("sp", None),
            P("sp", None),
            P("sp", None),
            P("sp", None, "tp"),
            P("sp", None, "tp"),
            P("sp", "tp", None),
            P(None, "tp"),
            P("sp", "tp"),
            P("sp", "tp"),
            P("sp", "tp"),
            P(None, "tp"),
            P("tp", None, None),
            P("tp", None, None),
            P("tp"),
            P("sp", "tp"),
        ),
        out_specs=(
            P("sp", None, "tp"),
            P("sp", None, "tp"),
            P("sp", "tp", None),
            P("sp", "tp"),
            P("sp", None),
            P("sp", "tp"),
            P("sp", "tp"),
        ),
        check_vma=False,
    )
```

```python
import functools

import jax
import jax.numpy as jnp
from jax import lax
from jax.experimental import pallas as pl
from jax.experimental.pallas import tpu as pltpu
from jax.sharding import PartitionSpec as P

decay_scale = 8.0
BF = jnp.bfloat16
F32 = jnp.float32
PLANES = 4
SEGMENTS = 8
LANES = 128
MESH = pl.DeviceIdType.MESH


def dot_nn(left, right):
    return jnp.dot(left, right, preferred_element_type=F32)


def dot_nt(left, right):
    return lax.dot_general(left, right, (((1,), (1,)), ((), ())), preferred_element_type=F32)


def dot_tn(left, right):
    return lax.dot_general(left, right, (((0,), (0,)), ((), ())), preferred_element_type=F32)


def aligned(index, size):
    return pl.ds(pl.multiple_of(index * size, size), size)


def local_wait(view, sem):
    pltpu.make_async_copy(view, view, sem).wait()


def remote(src, dst, send, recv, **where):
    return pltpu.make_async_remote_copy(
        src_ref=src, dst_ref=dst, send_sem=send, recv_sem=recv, device_id=where, device_id_type=MESH
    )


def iota(shape, axis):
    return lax.broadcasted_iota(jnp.int32, shape, axis)


def fallen(rise):
    series = 1.0 - rise * (1.0 / 7.0)
    for order in range(6, 1, -1):
        series = 1.0 - rise * (1.0 / order) * series
    return jnp.where(rise < 0.25, rise * series, 1.0 - jnp.exp(-rise))


def whole_kernel(
    count, cap,
    tok_ref, cot_ref, ids_ref, route_ref, decay_w, input_w, taps_in, rate_ref,
    gate_w, up_w, down_w, out_w, recur_in, gate_in, states_in, extra_in,
    gate_g, up_g, down_g, weight_out, grad_ref, recur_out, gate_out, plane_ref,
    wgu, wd, table, slot_scale, near_tok, near_cot, far_tok, far_cot, far_ids, far_route, far_moe,
    send_r, send_g, rg, pre, hid, xgu, own, psend, precv, back, halves,
    cols, send_part, got_part, gelu, slope, first, second, third, decays, cumul, local,
    taps_ref, edge, shifted, prev_in, prev_state, pieces, plane_pair, plane_pieces, products,
    load_sem, bulk_sem, rows_sem, grads_sem, back_sem, mixer_sem, pair_send, pair_recv,
    before_sem, cols_sem, part_sem, carry_recv, plane_send, plane_recv, halo_sem, far_send, far_recv,
):
    me, core = lax.axis_index("sp"), lax.axis_index("tp")
    other = 1 - core
    peers = count // PLANES
    zed, pos = me // peers, lax.rem(me, peers)
    group = peers * cap
    tokens, width = tok_ref.shape
    slots = count * cap
    half = width // 2
    hidden = wd.shape[0]
    channels = states_in.shape[1]
    blocks = channels // LANES
    segment_rows = tokens // SEGMENTS
    mine, theirs = aligned(core, half), aligned(other, half)
    deep = PLANES // 2
    base = zed // deep * deep
    far = lax.rem(zed + deep, PLANES) * peers + pos
    near_slots = slots // 2
    conv_grad = own.at[0]
    mixer = send_part.at[pl.ds(0, tokens)]
    rows, grads = rg.at[pl.ds(0, 2)], rg.at[pl.ds(2, 2)]

    loads = [
        pltpu.make_async_copy(gate_w, wgu.at[:, pl.ds(0, hidden)], load_sem.at[0]),
        pltpu.make_async_copy(up_w, wgu.at[:, pl.ds(hidden, hidden)], load_sem.at[1]),
        pltpu.make_async_copy(down_w, wd, load_sem.at[2]),
    ]
    inputs = [
        pltpu.make_async_copy(states_in, own.at[0], load_sem.at[3]),
        pltpu.make_async_copy(extra_in, own.at[1], load_sem.at[4]),
        pltpu.make_async_copy(recur_in, psend.at[0], load_sem.at[5]),
        pltpu.make_async_copy(gate_in, psend.at[1], load_sem.at[6]),
    ]
    near_loads = [
        pltpu.make_async_copy(tok_ref.at[:, mine], near_tok, load_sem.at[7]),
        pltpu.make_async_copy(cot_ref.at[:, mine], near_cot, load_sem.at[8]),
    ]
    for load in near_loads + inputs + loads:
        load.start()

    barrier = pltpu.get_barrier_semaphore()

    def greet(step, carry):
        pl.semaphore_signal(
            barrier, inc=1, device_id={"sp": lax.rem(me + step, count)}, device_id_type=MESH
        )
        return carry

    lax.fori_loop(1, count, greet, 0)
    pl.semaphore_signal(barrier, inc=1, device_id={"tp": other}, device_id_type=MESH)

    def tabulate(kind, ids, route):
        expert = iota((LANES, tokens), 0) + base * peers
        chosen = [ids[k : k + 1, :] == expert for k in range(2)]
        inside = iota((LANES, tokens), 0) < deep * peers
        member = jnp.where((chosen[0] | chosen[1]) & inside, 1.0, 0.0).astype(BF)
        earlier = (iota((tokens, tokens), 0) < iota((tokens, tokens), 1)).astype(F32).astype(BF)
        rank = dot_nn(member, earlier).astype(BF)
        low = iota((near_slots, LANES), 1) * cap
        row = iota((near_slots, LANES), 0)
        within = (row >= low) & (row < low + cap)
        widen = jnp.where(within, 1.0, 0.0).astype(BF)
        place_in = jnp.sum(jnp.where(within, (row - low).astype(F32), 0.0), axis=1, keepdims=True)
        taken = (dot_nn(widen, member) > 0.5) & (dot_nn(widen, rank) == place_in)
        table[kind] = jnp.where(taken, 1.0, 0.0).astype(BF)
        scale = jnp.where(chosen[0], route[0:1, :], 0.0) + jnp.where(chosen[1], route[1:2, :], 0.0)
        total = jnp.zeros((near_slots, tokens), F32)
        for _ in range(3):
            rounded = scale.astype(BF)
            total = total + dot_nn(widen, rounded)
            scale = scale - rounded.astype(F32)
        slot_scale[kind] = jnp.sum(jnp.where(taken, total, 0.0), axis=1, keepdims=True)

    taps_ref[...] = taps_in[...].astype(F32)
    tabulate(0, ids_ref[...], route_ref[...])
    pl.semaphore_wait(barrier, count)

    keep_rows = 16
    before = [
        remote(
            recur_in.at[pl.ds(tokens - keep_rows, keep_rows)], prev_in,
            before_sem.at[0], before_sem.at[1], sp=me + 1,
        ),
        remote(
            states_in.at[pl.ds(tokens - 8, 8)], prev_state,
            before_sem.at[2], before_sem.at[3], sp=me + 1,
        ),
    ]

    @pl.when(me < count - 1)
    def _():
        for copy in before:
            copy.start()

    to_far = [
        remote(ids_ref, far_ids, far_send.at[0], far_recv.at[0], sp=far),
        remote(route_ref, far_route, far_send.at[1], far_recv.at[1], sp=far),
        remote(tok_ref.at[:, mine], far_tok, far_send.at[2], far_recv.at[2], sp=far),
        remote(cot_ref.at[:, mine], far_cot, far_send.at[3], far_recv.at[3], sp=far),
    ]
    for copy in to_far:
        copy.start()

    def spread(level, source, target, which, sem):
        plane = base + level

        def one(shift, carry):
            spot = lax.rem(pos + shift, peers)
            remote(
                source(plane * peers + spot), target, bulk_sem.at[which], sem,
                sp=plane * peers + spot,
            ).start()
            return carry

        here = plane == zed
        lax.fori_loop(jnp.where(here, 1, 0), peers, one, 0)

        @pl.when(here)
        def _():
            pltpu.make_async_copy(source(me), target, sem).start()

    def dispatch(kind, which):
        tokens_in = (
            (near_tok, near_cot) if kind == 0 else (far_tok, far_cot)
        )[which]
        sent = (send_r, send_g)[which]
        target = (rows, grads)[which]
        sems = (rows_sem, grads_sem)[which]
        origin = me if kind == 0 else far
        plane_of = zed if kind == 0 else lax.rem(zed + deep, PLANES)

        def issue(step, carry):
            level = lax.rem(zed - base + 1 + step, deep)
            span = aligned(level, group)
            placed = dot_nn(table[kind, span, :], tokens_in[...])
            if which == 1:
                placed = placed * slot_scale[kind, span, :]
            sent[kind, span, :] = placed.astype(BF)
            spread(
                level,
                lambda dest: sent.at[kind, aligned(dest - base * peers, cap)],
                target.at[core, aligned(origin, cap)], which + 7 * kind * (1 - which), sems.at[plane_of],
            )
            return carry

        lax.fori_loop(0, deep, issue, 0)

    near_loads[0].wait()
    dispatch(0, 0)
    near_loads[1].wait()
    dispatch(0, 1)

    for load in inputs:
        load.wait()

    @pl.when(me > 0)
    def _():
        for copy in before:
            copy.wait_recv()

    @pl.when(me == 0)
    def _():
        prev_in[...] = jnp.zeros_like(prev_in)
        prev_state[...] = jnp.zeros_like(prev_state)

    def recurrence(block, carry):
        at = aligned(block, LANES)
        states = own[0, :, at]
        gate = psend[1, :, at].astype(F32)
        value, back_of = jax.vjp(functools.partial(jax.nn.gelu, approximate=True), gate)
        mixer[:, at] = (states * value).astype(BF)
        gelu[:, at] = value
        slope[:, at] = states * back_of(jnp.ones_like(value))[0]
        shifted[0:8, :] = prev_in[8:16, at].astype(F32)
        shifted[8:, :] = psend[0, :, at].astype(F32)
        conv = taps_ref[0:1, at] * shifted[5 : 5 + tokens, :]
        for tap in range(1, 4):
            conv = conv + taps_ref[tap : tap + 1, at] * shifted[5 + tap : 5 + tap + tokens, :]
        maps = jnp.concatenate([decay_w[block], input_w[block]], axis=1)
        gates = jax.nn.sigmoid(dot_nn(conv.astype(BF), maps))
        recur_gate, input_gate = gates[:, :LANES], gates[:, LANES:]
        rate = -decay_scale * rate_ref[0:1, at]
        log_decay = rate * recur_gate + own[1, :, at]
        decay = jnp.exp(log_decay)
        opening = (iota((tokens, LANES), 0) == 0) & (me == 0)
        mult = jnp.where(opening, 1.0, jnp.sqrt(fallen(-2.0 * log_decay)))
        shifted[0:8, :] = prev_state[:, at]
        shifted[8:, :] = states
        fall = jnp.where(opening, 0.0, input_gate * conv * decay * decay / mult)
        factor = shifted[7 : 7 + tokens, :] * decay - fall
        first[:, at] = factor * rate * recur_gate * (1.0 - recur_gate)
        third_value = mult * input_gate
        second[:, at] = third_value * conv * (1.0 - input_gate)
        third[:, at] = third_value
        decays[block] = decay

        def along(step, carry):
            product, decay = carry
            picked = pl.ds(segment_rows - 1 - step, SEGMENTS, stride=segment_rows)
            product = product * decay
            cumul[block, picked, :] = product
            return product, decays[block, picked, :]

        picked = pl.ds(segment_rows - 1, SEGMENTS, stride=segment_rows)
        decay = decays[block, picked, :]
        product = decay * 0.0 + 1.0
        cumul[block, picked, :] = product
        product, decay = lax.fori_loop(1, segment_rows, along, (product, decay))
        products[:, at] = product * decay
        return carry

    lax.fori_loop(0, blocks, recurrence, 0)

    to_far[0].wait_recv()
    to_far[1].wait_recv()
    tabulate(1, far_ids[...], far_route[...])
    to_far[2].wait_recv()
    dispatch(1, 0)

    def from_plane(step):
        return lax.rem(base + deep * (step // deep) + lax.rem(zed - base + step, deep), PLANES)

    def to_pair(view, slot):
        return remote(view, view, pair_send.at[slot], pair_recv.at[slot], tp=other)

    def pass_rows(step, carry):
        plane = from_plane(step)
        view = rows.at[core, aligned(plane, group)]
        local_wait(view, rows_sem.at[plane])
        to_pair(view, step).start()
        return carry

    lax.fori_loop(0, deep, pass_rows, 0)
    for load in loads:
        load.wait()

    def forward(step, carry):
        span = aligned(from_plane(step), group)
        to_pair(rows.at[other, span], step).wait_recv()
        pre[span, :] = dot_nn(rows[0, span, :], wgu[:half, :]) + dot_nn(
            rows[1, span, :], wgu[half:, :]
        )
        return carry

    lax.fori_loop(0, deep, forward, 0)
    to_far[3].wait_recv()
    dispatch(1, 1)
    near_bytes = precv.at[pl.ds(0, (deep * peers - 1) * cap)]
    sent_bytes = precv.at[pl.ds(0, 2 * (deep * peers - 1) * cap)]
    local_wait(near_bytes, bulk_sem.at[0])

    def finish(step):
        plane = from_plane(step)
        span = aligned(plane, group)
        to_pair(precv.at[span], 2 * PLANES + step).wait_recv()
        kind = step // deep
        level = lax.rem(plane, deep)
        near = aligned(level, group)
        send_r[kind, near, :] = (own[lax.rem(step, 2)] + precv[span, :].astype(F32)).astype(BF)

    def release(step):
        kind, level = step // deep, lax.rem(from_plane(step), deep)
        spread(
            level,
            lambda dest: send_r.at[kind, aligned(dest - base * peers, cap)],
            back.at[kind, aligned(me - base * peers, cap)], 2, back_sem.at[kind * deep + zed - base],
        )

    def swap_part(step, span):
        return remote(
            psend.at[lax.rem(step, 2)], precv.at[span], pair_send.at[2 * PLANES + step],
            pair_recv.at[2 * PLANES + step], tp=other,
        )

    def backward(step, eager):
        plane = from_plane(step)
        span = aligned(plane, group)
        view = grads.at[core, span]
        local_wait(view, grads_sem.at[plane])
        to_pair(view, PLANES + step).start()

        @pl.when(lax.rem(step, deep) > 0)
        def _():
            finish(step - 1)
            if eager:
                release(step - 1)

        to_pair(grads.at[other, span], PLANES + step).wait_recv()
        hidden_grad = dot_nt(grads[0, span, :], wd[:, :half]) + dot_nt(
            grads[1, span, :], wd[:, half:]
        )
        gate = pre[span, :hidden]
        up = pre[span, hidden:]
        sig = jax.nn.sigmoid(gate)
        silu = gate * sig
        hid[span, :] = (silu * up).astype(BF)
        xgu[span, :hidden] = (hidden_grad * up * sig * (1.0 + gate * (1.0 - sig))).astype(BF)
        xgu[span, hidden:] = (hidden_grad * silu).astype(BF)

        @pl.when(step > 1)
        def _():
            swap_part(step - 2, span).wait_send()

        psend[lax.rem(step, 2)] = dot_nt(xgu[span, :], wgu[theirs, :]).astype(BF)
        swap_part(step, span).start()
        own[lax.rem(step, 2)] = dot_nt(xgu[span, :], wgu[mine, :])

    def quiet_backward(step, carry):
        backward(step, False)
        return carry

    def eager_backward(step, carry):
        backward(step, True)
        return carry

    def late_release(step, carry):
        release(step)
        return carry

    lax.fori_loop(0, deep, quiet_backward, 0)
    finish(deep - 1)
    lax.fori_loop(deep, PLANES, pass_rows, 0)
    lax.fori_loop(deep, PLANES, forward, 0)
    local_wait(near_bytes, bulk_sem.at[7])
    lax.fori_loop(deep, PLANES, eager_backward, 0)
    finish(PLANES - 1)
    release(PLANES - 1)
    lax.fori_loop(0, deep, late_release, 0)

    def share(shift, carry):
        dest = zed * peers + lax.rem(pos + shift, peers)
        remote(
            mixer, plane_ref.at[aligned(pos, tokens)], bulk_sem.at[3], mixer_sem.at[0], sp=dest
        ).start()
        return carry

    lax.fori_loop(1, peers, share, 0)
    keep = pltpu.make_async_copy(mixer, plane_ref.at[aligned(pos, tokens)], mixer_sem.at[1])
    keep.start()

    out_load = pltpu.make_async_copy(out_w, wgu, load_sem.at[0])
    out_load.start()

    tile = 256

    def weigh(side):
        def weight_tile(step, carry):
            columns = aligned(step, tile)
            spot = pl.ds(pl.multiple_of(side * half + step * tile, tile), tile)
            both = dot_tn(rows[side, :, columns], xgu[...]).astype(BF)
            gate_g[spot, :] = both[:, :hidden]
            up_g[spot, :] = both[:, hidden:]
            down_g[:, spot] = dot_tn(hid[...], grads[side, :, columns]).astype(BF)
            return carry

        lax.fori_loop(0, half // tile, weight_tile, 0)

    weigh(0)

    def gather(step, carry):
        kind, level = step // deep, lax.rem(step, deep)
        local_wait(back.at[kind, aligned(level, group)], back_sem.at[step])
        return carry

    lax.fori_loop(deep, PLANES, gather, 0)
    far_tok[...] = dot_tn(table[1], back[1]).astype(BF)
    far_sum = remote(far_tok, far_moe, far_send.at[4], far_recv.at[4], sp=far)
    far_sum.start()
    weigh(1)
    for slot in range(2 * PLANES):
        to_pair(rows.at[0, pl.ds(0, group)], slot).wait_send()
    shared = plane_ref.at[pl.ds(0, (peers - 1) * tokens)]
    local_wait(shared, mixer_sem.at[0])
    keep.wait()
    local_wait(shared, bulk_sem.at[3])
    chunks = peers * tokens // slots
    mixer_loads = [
        pltpu.make_async_copy(
            plane_ref.at[pl.ds(chunk * slots, slots)], rg.at[chunk], load_sem.at[1 + chunk]
        )
        for chunk in range(chunks)
    ]
    for load in mixer_loads:
        load.start()

    lax.fori_loop(0, deep, gather, 0)
    moe = dot_tn(table[0], back[0]) + near_cot[...].astype(F32)
    far_sum.wait_recv()
    halves[core] = (moe + far_moe[...].astype(F32)).astype(BF)
    last = to_pair(halves.at[core], 3 * PLANES)
    last.start()

    cut = width // count
    lane = cols.shape[1] // PLANES

    def column_block(level, place):
        return aligned((level * peers + place) * cut // lane, lane)

    def send_cols(shift, carry):
        place = lax.rem(pos + shift, peers)
        for level in range(deep):
            remote(
                halves.at[core, :, column_block(level, place)],
                cols.at[aligned(pos, tokens), aligned(core * deep + level, lane)],
                bulk_sem.at[4], cols_sem.at[0], sp=zed * peers + place,
            ).start()
        return carry

    lax.fori_loop(1, peers, send_cols, 0)
    kept = [
        pltpu.make_async_copy(
            halves.at[core, :, column_block(level, pos)],
            cols.at[aligned(pos, tokens), aligned(core * deep + level, lane)],
            cols_sem.at[1 + level],
        )
        for level in range(deep)
    ]
    for copy in kept:
        copy.start()

    grad_ref[:, mine] = halves[core]
    out_load.wait()
    to_pair(halves.at[other], 3 * PLANES).wait_recv()
    grad_ref[:, theirs] = halves[other]

    mixer_grad = dot_nn(halves[0], wgu[:half, :]) + dot_nn(halves[1], wgu[half:, :])
    gate_out[...] = (mixer_grad * slope[...]).astype(BF)
    for block in range(blocks):
        at = pl.ds(block * LANES, LANES)
        local[block] = mixer_grad[:, block * LANES : (block + 1) * LANES] * gelu[:, at]

    def scan(step, carry):
        picked = pl.ds(segment_rows - 1 - step, SEGMENTS, stride=segment_rows)
        after = []
        for block in range(blocks):
            total, decay = carry[block]
            total = local[block, picked, :] + decay * total
            local[block, picked, :] = total
            after.append((total, decays[block, picked, :]))
        return after

    picked = pl.ds(segment_rows - 1, SEGMENTS, stride=segment_rows)
    start = [(local[block, picked, :], decays[block, picked, :]) for block in range(blocks)]
    ended = lax.fori_loop(1, segment_rows, scan, start)
    total = jnp.concatenate([piece[0] * piece[1] for piece in ended], axis=1)
    product = products[...]
    whole, entry = product[SEGMENTS - 1 :], total[SEGMENTS - 1 :]
    for segment in range(SEGMENTS - 2, -1, -1):
        row = slice(segment, segment + 1)
        whole = whole * product[row]
        entry = total[row] + product[row] * entry
    pieces[pos, 0:1, :] = whole
    pieces[pos, 1:2, :] = entry

    def send_carry(shift, carry):
        dest = zed * peers + lax.rem(pos + shift, peers)
        remote(pieces.at[pos], pieces.at[pos], bulk_sem.at[6], carry_recv.at[pos], sp=dest).start()
        return carry

    lax.fori_loop(1, peers, send_carry, 0)

    def wait_carry(shift, carry):
        source = lax.rem(pos + shift, peers)
        local_wait(pieces.at[source], carry_recv.at[source])
        return carry

    lax.fori_loop(1, peers, wait_carry, 0)
    blank = whole * 0.0
    whole, entry = blank + 1.0, blank
    after, after_entry = whole, entry
    for spot in range(peers - 1, -1, -1):
        factor, addend = pieces[spot, 0:1, :], pieces[spot, 1:2, :]
        whole = factor * whole
        entry = addend + factor * entry
        later = spot > pos
        after = jnp.where(later, factor * after, after)
        after_entry = jnp.where(later, addend + factor * after_entry, after_entry)
    plane_pair[0:1, :] = whole
    plane_pair[1:2, :] = entry

    def plane_copy(plane):
        return remote(
            plane_pair, plane_pieces.at[zed], plane_send.at[plane], plane_recv.at[zed],
            sp=plane * peers + pos,
        )

    def send_plane(step, carry):
        plane_copy(zed - 1 - step).start()
        return carry

    lax.fori_loop(0, zed, send_plane, 0)

    local_wait(cols.at[pl.ds(0, (peers - 1) * tokens), pl.ds(0, deep * lane)], cols_sem.at[0])
    for copy in kept:
        copy.wait()
    cols_mine = cols.at[:, aligned(core, deep * lane)]
    cols_pass = to_pair(cols_mine, 3 * PLANES + 1)
    cols_pass.start()

    for load in mixer_loads:
        load.wait()
    to_pair(cols.at[:, aligned(other, deep * lane)], 3 * PLANES + 1).wait_recv()
    sums = pl.ds(0, PLANES * lane)
    partial = dot_tn(cols[pl.ds(0, slots), :], rg[0])
    for chunk in range(1, chunks):
        partial = partial + dot_tn(cols[pl.ds(chunk * slots, slots), :], rg[chunk])
    pre[sums, :] = partial
    send_part[...] = partial.astype(BF)

    def part_rows(plane):
        offset = lax.rem((plane * peers + pos) * cut, lane)
        return pl.ds(pl.multiple_of(plane * lane + offset, cut), cut)

    def send_block(shift, carry):
        plane = lax.rem(zed + shift, PLANES)
        remote(
            send_part.at[part_rows(plane)], got_part.at[aligned(zed, cut)],
            bulk_sem.at[5], part_sem.at[zed], sp=plane * peers + pos,
        ).start()
        return carry

    lax.fori_loop(1, PLANES, send_block, 0)

    def take_plane(step, entering):
        source = PLANES - 1 - step
        local_wait(plane_pieces.at[source], plane_recv.at[source])
        return plane_pieces[source, 0:1, :] * entering + plane_pieces[source, 1:2, :]

    entering = lax.fori_loop(0, PLANES - 1 - zed, take_plane, blank)
    entering = after_entry + after * entering
    enter = []
    for segment in range(SEGMENTS - 1, -1, -1):
        enter.append(entering)
        row = slice(segment, segment + 1)
        entering = total[row] + product[row] * entering
    enter = jnp.concatenate(enter[::-1], axis=0)

    for block in range(blocks):
        at = slice(block * LANES, (block + 1) * LANES)
        filled = jnp.broadcast_to(enter[:, None, at], (SEGMENTS, segment_rows, LANES))
        carried = local[block] + cumul[block] * filled.reshape(tokens, LANES)
        both = jnp.concatenate(
            [(carried * first[:, at]).astype(BF), (carried * second[:, at]).astype(BF)], axis=1
        )
        maps = jnp.concatenate([decay_w[block], input_w[block]], axis=1)
        conv_grad[0:tokens, at] = carried * third[:, at] + dot_nt(both, maps)

    halo = pl.ds(16, 8)
    halo_copy = remote(
        conv_grad.at[pl.ds(0, 8)], edge.at[halo], halo_sem.at[0], halo_sem.at[1], sp=me - 1
    )

    @pl.when(me > 0)
    def _():
        halo_copy.start()

    @pl.when(me == count - 1)
    def _():
        edge[halo, :] = jnp.zeros((8, channels), F32)

    edge[0:16, :] = conv_grad[tokens - 16 : tokens, :]

    def taps_over(source, rows):
        total = taps_ref[0:1, :] * source[3 : rows + 3, :]
        for tap in range(1, 4):
            total = total + taps_ref[tap : tap + 1, :] * source[3 - tap : rows + 3 - tap, :]
        return total.astype(BF)

    recur_out[0 : tokens - 16, :] = taps_over(conv_grad, tokens - 16)

    @pl.when(me < count - 1)
    def _():
        local_wait(edge.at[halo], halo_sem.at[1])

    recur_out[tokens - 16 : tokens, :] = taps_over(edge, 16)

    summed = pre[part_rows(zed), :]
    for shift in range(1, PLANES):
        plane = lax.rem(zed + shift, PLANES)
        local_wait(got_part.at[aligned(plane, cut)], part_sem.at[plane])
        summed = summed + got_part[aligned(plane, cut), :].astype(F32)
    weight_out[...] = summed

    for which in (1, 2):
        local_wait(sent_bytes, bulk_sem.at[which])
    local_wait(pieces.at[pl.ds(0, peers - 1)], bulk_sem.at[6])
    for copy in to_far:
        copy.wait_send()
    far_sum.wait_send()
    local_wait(cols.at[pl.ds(0, (peers - 1) * tokens), pl.ds(0, deep * lane)], bulk_sem.at[4])
    local_wait(got_part.at[pl.ds(0, (PLANES - 1) * cut)], bulk_sem.at[5])
    for step in range(PLANES - 2, PLANES):
        swap_part(step, pl.ds(0, group)).wait_send()
    last.wait_send()
    cols_pass.wait_send()

    def sent_plane(step, carry):
        plane_copy(zed - 1 - step).wait_send()
        return carry

    lax.fori_loop(0, zed, sent_plane, 0)

    @pl.when(me > 0)
    def _():
        halo_copy.wait_send()

    @pl.when(me < count - 1)
    def _():
        for copy in before:
            copy.wait_send()


def flush_kernel(total, *refs):
    sems = refs[-1]
    copies = [
        pltpu.make_async_copy(refs[item], refs[total + item], sems.at[item])
        for item in range(total)
    ]
    for copy in copies:
        copy.start()
    for copy in copies:
        copy.wait()


def flushed(*results):
    total = len(results)
    size = sum(result.size * result.dtype.itemsize for result in results)
    return pl.pallas_call(
        functools.partial(flush_kernel, total),
        in_specs=[pl.BlockSpec(memory_space=pltpu.VMEM)] * total,
        out_specs=[pl.BlockSpec(memory_space=pl.ANY)] * total,
        out_shape=[jax.ShapeDtypeStruct(result.shape, result.dtype) for result in results],
        scratch_shapes=[pltpu.SemaphoreType.DMA((total,))],
        compiler_params=pltpu.CompilerParams(vmem_limit_bytes=4 * 1024 * 1024),
        cost_estimate=pl.CostEstimate(flops=1000, bytes_accessed=2 * size, transcendentals=0),
        name="flush",
    )(*results)


def on_device(
    moe_input,
    cotangent,
    expert_ids,
    route_weight,
    gate_proj,
    up_proj,
    down_proj,
    out_weight,
    recur_input,
    gate_input,
    states,
    conv_taps,
    decay_gate_w,
    input_gate_w,
    decay_rate,
    decay_extra,
):
    count = lax.axis_size("sp")
    tokens, width = moe_input.shape
    cap = max(2, 4 * tokens // count)
    slots = count * cap
    half = width // 2
    hidden = gate_proj.shape[2]
    channels = states.shape[1]
    peers = count // PLANES
    group = peers * cap
    cut = width // count
    lane = max(cut, LANES)
    blocks = channels // LANES
    vmem, anywhere = pl.BlockSpec(memory_space=pltpu.VMEM), pl.BlockSpec(memory_space=pl.ANY)
    dma = pltpu.SemaphoreType.DMA

    def out(shape, kind):
        return pltpu.VMEM(shape, kind)

    def plain(kind):
        return pltpu.VMEM((tokens, channels), kind)

    results = pl.pallas_call(
        functools.partial(whole_kernel, count, cap),
        in_specs=[anywhere] * 2 + [vmem] * 6 + [anywhere] * 8,
        out_specs=[vmem] * 7 + [anywhere],
        out_shape=[
            out((width, hidden), BF), out((width, hidden), BF), out((hidden, width), BF),
            out((cut, channels), F32), out((tokens, width), BF), out((tokens, channels), BF),
            out((tokens, channels), BF), jax.ShapeDtypeStruct((peers * tokens, channels), BF),
        ],
        scratch_shapes=[
            pltpu.VMEM((width, 2 * hidden), BF),
            pltpu.VMEM((hidden, width), BF),
            pltpu.VMEM((2, slots // 2, tokens), BF),
            pltpu.VMEM((2, slots // 2, 1), F32),
            pltpu.VMEM((tokens, half), BF),
            pltpu.VMEM((tokens, half), BF),
            pltpu.VMEM((tokens, half), BF),
            pltpu.VMEM((tokens, half), BF),
            pltpu.VMEM((2, tokens), jnp.int32),
            pltpu.VMEM((2, tokens), F32),
            pltpu.VMEM((tokens, half), BF),
            pltpu.VMEM((2, slots // 2, half), BF),
            pltpu.VMEM((2, slots // 2, half), BF),
            pltpu.VMEM((4, slots, half), BF),
            pltpu.VMEM((slots, 2 * hidden), F32),
            pltpu.VMEM((slots, hidden), BF),
            pltpu.VMEM((slots, 2 * hidden), BF),
            pltpu.VMEM((2, group, half), F32),
            pltpu.VMEM((2, group, half), BF),
            pltpu.VMEM((slots, half), BF),
            pltpu.VMEM((2, slots // 2, half), BF),
            pltpu.VMEM((2, tokens, half), BF),
            pltpu.VMEM((peers * tokens, PLANES * lane), BF),
            pltpu.VMEM((PLANES * lane, channels), BF),
            pltpu.VMEM((PLANES * cut, channels), BF),
            plain(F32), plain(F32), plain(F32), plain(F32), plain(F32),
            *[pltpu.VMEM((blocks, tokens, LANES), F32)] * 3,
            pltpu.VMEM((4, channels), F32),
            pltpu.VMEM((24, channels), F32),
            pltpu.VMEM((tokens + 8, LANES), F32),
            pltpu.VMEM((16, channels), BF),
            pltpu.VMEM((8, channels), F32),
            pltpu.VMEM((peers, 2, channels), F32),
            pltpu.VMEM((2, channels), F32),
            pltpu.VMEM((PLANES, 2, channels), F32),
            pltpu.VMEM((SEGMENTS, channels), F32),
            dma((9,)), dma((8,)), dma((PLANES,)), dma((PLANES,)), dma((PLANES,)), dma((2,)),
            dma((3 * PLANES + 2,)), dma((3 * PLANES + 2,)), dma((4,)), dma((3,)), dma((PLANES,)),
            dma((peers,)), dma((PLANES,)), dma((PLANES,)), dma((2,)), dma((5,)), dma((5,)),
        ],
        compiler_params=pltpu.CompilerParams(
            collective_id=0, has_side_effects=True, vmem_limit_bytes=54 * 1024 * 1024
        ),
        cost_estimate=pl.CostEstimate(
            flops=16 * slots * width * hidden, bytes_accessed=40 << 20, transcendentals=0
        ),
        name="whole",
    )(
        moe_input, cotangent, expert_ids.T, route_weight.T, decay_gate_w, input_gate_w,
        conv_taps, decay_rate[None], gate_proj[0], up_proj[0], down_proj[0], out_weight,
        recur_input, gate_input, states, decay_extra,
    )
    gate_g, up_g, down_g, weight_g, grad, recur_g, gate_in_g = flushed(*results[:7])
    return (gate_g[None], up_g[None], down_g[None], weight_g, grad, recur_g, gate_in_g)


def solution(mesh):
    return jax.shard_map(
        on_device,
        mesh=mesh,
        in_specs=(
            P("sp", None),
            P("sp", None),
            P("sp", None),
            P("sp", None),
            P("sp", None, "tp"),
            P("sp", None, "tp"),
            P("sp", "tp", None),
            P(None, "tp"),
            P("sp", "tp"),
            P("sp", "tp"),
            P("sp", "tp"),
            P(None, "tp"),
            P("tp", None, None),
            P("tp", None, None),
            P("tp"),
            P("sp", "tp"),
        ),
        out_specs=(
            P("sp", None, "tp"),
            P("sp", None, "tp"),
            P("sp", "tp", None),
            P("sp", "tp"),
            P("sp", None),
            P("sp", "tp"),
            P("sp", "tp"),
        ),
        check_vma=False,
    )
```

```python
import functools

import jax
import jax.numpy as jnp
from jax import lax
from jax.experimental import pallas as pl
from jax.experimental.pallas import tpu as pltpu
from jax.sharding import PartitionSpec as P

decay_scale = 8.0
BF = jnp.bfloat16
F32 = jnp.float32
PLANES = 4
SEGMENTS = 8
LANES = 128
MESH = pl.DeviceIdType.MESH


def dot_nn(left, right):
    return jnp.dot(left, right, preferred_element_type=F32)


def dot_nt(left, right):
    return lax.dot_general(left, right, (((1,), (1,)), ((), ())), preferred_element_type=F32)


def dot_tn(left, right):
    return lax.dot_general(left, right, (((0,), (0,)), ((), ())), preferred_element_type=F32)


def aligned(index, size):
    return pl.ds(pl.multiple_of(index * size, size), size)


def local_wait(view, sem):
    pltpu.make_async_copy(view, view, sem).wait()


def remote(src, dst, send, recv, **where):
    return pltpu.make_async_remote_copy(
        src_ref=src, dst_ref=dst, send_sem=send, recv_sem=recv, device_id=where, device_id_type=MESH
    )


def iota(shape, axis):
    return lax.broadcasted_iota(jnp.int32, shape, axis)


def fallen(rise):
    series = 1.0 - rise * (1.0 / 7.0)
    for order in range(6, 1, -1):
        series = 1.0 - rise * (1.0 / order) * series
    return jnp.where(rise < 0.25, rise * series, 1.0 - jnp.exp(-rise))


def whole_kernel(
    count, cap,
    tok_ref, cot_ref, ids_ref, route_ref, decay_w, input_w, taps_in, rate_ref,
    gate_w, up_w, down_w, out_w, recur_in, gate_in, states_in, extra_in,
    gate_g, up_g, down_g, weight_out, grad_ref, recur_out, gate_out, plane_ref,
    wgu, wd, table, slot_scale, near_tok, near_cot, far_tok, far_cot, far_ids, far_route, far_moe,
    send_r, send_g, rg, pre, hid, xgu, own, psend, precv, back, halves,
    cols, send_part, got_part, gelu, slope, first, second, third, decays, cumul, local,
    taps_ref, edge, shifted, prev_in, prev_state, pieces, plane_pair, plane_pieces, products,
    load_sem, bulk_sem, rows_sem, grads_sem, back_sem, mixer_sem, pair_send, pair_recv,
    before_sem, cols_sem, part_sem, carry_recv, plane_send, plane_recv, halo_sem, far_send, far_recv,
):
    me, core = lax.axis_index("sp"), lax.axis_index("tp")
    other = 1 - core
    peers = count // PLANES
    zed, pos = me // peers, lax.rem(me, peers)
    group = peers * cap
    tokens, width = tok_ref.shape
    slots = count * cap
    half = width // 2
    hidden = wd.shape[0]
    channels = states_in.shape[1]
    blocks = channels // LANES
    segment_rows = tokens // SEGMENTS
    mine, theirs = aligned(core, half), aligned(other, half)
    deep = PLANES // 2
    base = zed // deep * deep
    far = lax.rem(zed + deep, PLANES) * peers + pos
    near_slots = slots // 2
    conv_grad = own.at[0]
    mixer = send_part.at[pl.ds(0, tokens)]
    rows, grads = rg.at[pl.ds(0, 2)], rg.at[pl.ds(2, 2)]

    loads = [
        pltpu.make_async_copy(gate_w, wgu.at[:, pl.ds(0, hidden)], load_sem.at[0]),
        pltpu.make_async_copy(up_w, wgu.at[:, pl.ds(hidden, hidden)], load_sem.at[1]),
        pltpu.make_async_copy(down_w, wd, load_sem.at[2]),
    ]
    inputs = [
        pltpu.make_async_copy(states_in, own.at[0], load_sem.at[3]),
        pltpu.make_async_copy(extra_in, own.at[1], load_sem.at[4]),
        pltpu.make_async_copy(recur_in, psend.at[0], load_sem.at[5]),
        pltpu.make_async_copy(gate_in, psend.at[1], load_sem.at[6]),
    ]
    near_loads = [
        pltpu.make_async_copy(tok_ref.at[:, mine], near_tok, load_sem.at[7]),
        pltpu.make_async_copy(cot_ref.at[:, mine], near_cot, load_sem.at[8]),
    ]
    for load in near_loads + inputs + loads:
        load.start()

    barrier = pltpu.get_barrier_semaphore()

    def greet(step, carry):
        pl.semaphore_signal(
            barrier, inc=1, device_id={"sp": lax.rem(me + step, count)}, device_id_type=MESH
        )
        return carry

    lax.fori_loop(1, count, greet, 0)
    pl.semaphore_signal(barrier, inc=1, device_id={"tp": other}, device_id_type=MESH)

    def tabulate(kind, ids, route):
        expert = iota((LANES, tokens), 0) + base * peers
        chosen = [ids[k : k + 1, :] == expert for k in range(2)]
        inside = iota((LANES, tokens), 0) < deep * peers
        member = jnp.where((chosen[0] | chosen[1]) & inside, 1.0, 0.0).astype(BF)
        earlier = (iota((tokens, tokens), 0) < iota((tokens, tokens), 1)).astype(F32).astype(BF)
        rank = dot_nn(member, earlier).astype(BF)
        low = iota((near_slots, LANES), 1) * cap
        row = iota((near_slots, LANES), 0)
        within = (row >= low) & (row < low + cap)
        widen = jnp.where(within, 1.0, 0.0).astype(BF)
        place_in = jnp.sum(jnp.where(within, (row - low).astype(F32), 0.0), axis=1, keepdims=True)
        taken = (dot_nn(widen, member) > 0.5) & (dot_nn(widen, rank) == place_in)
        table[kind] = jnp.where(taken, 1.0, 0.0).astype(BF)
        scale = jnp.where(chosen[0], route[0:1, :], 0.0) + jnp.where(chosen[1], route[1:2, :], 0.0)
        total = jnp.zeros((near_slots, tokens), F32)
        for _ in range(3):
            rounded = scale.astype(BF)
            total = total + dot_nn(widen, rounded)
            scale = scale - rounded.astype(F32)
        slot_scale[kind] = jnp.sum(jnp.where(taken, total, 0.0), axis=1, keepdims=True)

    taps_ref[...] = taps_in[...].astype(F32)
    tabulate(0, ids_ref[...], route_ref[...])
    pl.semaphore_wait(barrier, count)

    keep_rows = 16
    before = [
        remote(
            recur_in.at[pl.ds(tokens - keep_rows, keep_rows)], prev_in,
            before_sem.at[0], before_sem.at[1], sp=me + 1,
        ),
        remote(
            states_in.at[pl.ds(tokens - 8, 8)], prev_state,
            before_sem.at[2], before_sem.at[3], sp=me + 1,
        ),
    ]

    @pl.when(me < count - 1)
    def _():
        for copy in before:
            copy.start()

    to_far = [
        remote(ids_ref, far_ids, far_send.at[0], far_recv.at[0], sp=far),
        remote(route_ref, far_route, far_send.at[1], far_recv.at[1], sp=far),
        remote(tok_ref.at[:, mine], far_tok, far_send.at[2], far_recv.at[2], sp=far),
        remote(cot_ref.at[:, mine], far_cot, far_send.at[3], far_recv.at[3], sp=far),
    ]
    for copy in to_far:
        copy.start()

    def spread(level, source, target, which, sem):
        plane = base + level

        def one(shift, carry):
            spot = lax.rem(pos + shift, peers)
            remote(
                source(plane * peers + spot), target, bulk_sem.at[which], sem,
                sp=plane * peers + spot,
            ).start()
            return carry

        here = plane == zed
        lax.fori_loop(jnp.where(here, 1, 0), peers, one, 0)

        @pl.when(here)
        def _():
            pltpu.make_async_copy(source(me), target, sem).start()

    def dispatch(kind, which):
        tokens_in = (
            (near_tok, near_cot) if kind == 0 else (far_tok, far_cot)
        )[which]
        sent = (send_r, send_g)[which]
        target = (rows, grads)[which]
        sems = (rows_sem, grads_sem)[which]
        origin = me if kind == 0 else far
        plane_of = zed if kind == 0 else lax.rem(zed + deep, PLANES)

        def issue(step, carry):
            level = lax.rem(zed - base + 1 + step, deep)
            span = aligned(level, group)
            placed = dot_nn(table[kind, span, :], tokens_in[...])
            if which == 1:
                placed = placed * slot_scale[kind, span, :]
            sent[kind, span, :] = placed.astype(BF)
            spread(
                level,
                lambda dest: sent.at[kind, aligned(dest - base * peers, cap)],
                target.at[core, aligned(origin, cap)], which + 7 * kind * (1 - which), sems.at[plane_of],
            )
            return carry

        lax.fori_loop(0, deep, issue, 0)

    near_loads[0].wait()
    dispatch(0, 0)
    near_loads[1].wait()
    dispatch(0, 1)

    for load in inputs:
        load.wait()

    @pl.when(me > 0)
    def _():
        for copy in before:
            copy.wait_recv()

    @pl.when(me == 0)
    def _():
        prev_in[...] = jnp.zeros_like(prev_in)
        prev_state[...] = jnp.zeros_like(prev_state)

    def recurrence(block, carry):
        at = aligned(block, LANES)
        states = own[0, :, at]
        gate = psend[1, :, at].astype(F32)
        value, back_of = jax.vjp(functools.partial(jax.nn.gelu, approximate=True), gate)
        mixer[:, at] = (states * value).astype(BF)
        gelu[:, at] = value
        slope[:, at] = states * back_of(jnp.ones_like(value))[0]
        shifted[0:8, :] = prev_in[8:16, at].astype(F32)
        shifted[8:, :] = psend[0, :, at].astype(F32)
        conv = taps_ref[0:1, at] * shifted[5 : 5 + tokens, :]
        for tap in range(1, 4):
            conv = conv + taps_ref[tap : tap + 1, at] * shifted[5 + tap : 5 + tap + tokens, :]
        maps = jnp.concatenate([decay_w[block], input_w[block]], axis=1)
        gates = jax.nn.sigmoid(dot_nn(conv.astype(BF), maps))
        recur_gate, input_gate = gates[:, :LANES], gates[:, LANES:]
        rate = -decay_scale * rate_ref[0:1, at]
        log_decay = rate * recur_gate + own[1, :, at]
        decay = jnp.exp(log_decay)
        opening = (iota((tokens, LANES), 0) == 0) & (me == 0)
        mult = jnp.where(opening, 1.0, jnp.sqrt(fallen(-2.0 * log_decay)))
        shifted[0:8, :] = prev_state[:, at]
        shifted[8:, :] = states
        fall = jnp.where(opening, 0.0, input_gate * conv * decay * decay / mult)
        factor = shifted[7 : 7 + tokens, :] * decay - fall
        first[:, at] = factor * rate * recur_gate * (1.0 - recur_gate)
        third_value = mult * input_gate
        second[:, at] = third_value * conv * (1.0 - input_gate)
        third[:, at] = third_value
        decays[block] = decay

        def along(step, carry):
            product, decay = carry
            picked = pl.ds(segment_rows - 1 - step, SEGMENTS, stride=segment_rows)
            product = product * decay
            cumul[block, picked, :] = product
            return product, decays[block, picked, :]

        picked = pl.ds(segment_rows - 1, SEGMENTS, stride=segment_rows)
        decay = decays[block, picked, :]
        product = decay * 0.0 + 1.0
        cumul[block, picked, :] = product
        product, decay = lax.fori_loop(1, segment_rows, along, (product, decay))
        products[:, at] = product * decay
        return carry

    lax.fori_loop(0, blocks, recurrence, 0)

    to_far[0].wait_recv()
    to_far[1].wait_recv()
    tabulate(1, far_ids[...], far_route[...])
    to_far[2].wait_recv()
    dispatch(1, 0)

    def from_plane(step):
        return lax.rem(base + deep * (step // deep) + lax.rem(zed - base + step, deep), PLANES)

    def to_pair(view, slot):
        return remote(view, view, pair_send.at[slot], pair_recv.at[slot], tp=other)

    def pass_rows(step, carry):
        plane = from_plane(step)
        view = rows.at[core, aligned(plane, group)]
        local_wait(view, rows_sem.at[plane])
        to_pair(view, step).start()
        return carry

    lax.fori_loop(0, deep, pass_rows, 0)
    for load in loads:
        load.wait()

    def forward(step, carry):
        span = aligned(from_plane(step), group)
        to_pair(rows.at[other, span], step).wait_recv()
        pre[span, :] = dot_nn(rows[0, span, :], wgu[:half, :]) + dot_nn(
            rows[1, span, :], wgu[half:, :]
        )
        return carry

    lax.fori_loop(0, deep, forward, 0)
    to_far[3].wait_recv()
    dispatch(1, 1)
    near_bytes = precv.at[pl.ds(0, (deep * peers - 1) * cap)]
    sent_bytes = precv.at[pl.ds(0, 2 * (deep * peers - 1) * cap)]
    local_wait(near_bytes, bulk_sem.at[0])

    def finish(step):
        plane = from_plane(step)
        span = aligned(plane, group)
        to_pair(precv.at[span], 2 * PLANES + step).wait_recv()
        kind = step // deep
        level = lax.rem(plane, deep)
        near = aligned(level, group)
        send_r[kind, near, :] = (own[lax.rem(step, 2)] + precv[span, :].astype(F32)).astype(BF)

    def release(step):
        kind, level = step // deep, lax.rem(from_plane(step), deep)
        spread(
            level,
            lambda dest: send_r.at[kind, aligned(dest - base * peers, cap)],
            back.at[kind, aligned(me - base * peers, cap)], 2, back_sem.at[kind * deep + zed - base],
        )

    def swap_part(step, span):
        return remote(
            psend.at[lax.rem(step, 2)], precv.at[span], pair_send.at[2 * PLANES + step],
            pair_recv.at[2 * PLANES + step], tp=other,
        )

    def backward(step, eager):
        plane = from_plane(step)
        span = aligned(plane, group)
        view = grads.at[core, span]
        local_wait(view, grads_sem.at[plane])
        to_pair(view, PLANES + step).start()

        @pl.when(lax.rem(step, deep) > 0)
        def _():
            finish(step - 1)
            if eager:
                release(step - 1)

        to_pair(grads.at[other, span], PLANES + step).wait_recv()
        hidden_grad = dot_nt(grads[0, span, :], wd[:, :half]) + dot_nt(
            grads[1, span, :], wd[:, half:]
        )
        gate = pre[span, :hidden]
        up = pre[span, hidden:]
        sig = jax.nn.sigmoid(gate)
        silu = gate * sig
        hid[span, :] = (silu * up).astype(BF)
        xgu[span, :hidden] = (hidden_grad * up * sig * (1.0 + gate * (1.0 - sig))).astype(BF)
        xgu[span, hidden:] = (hidden_grad * silu).astype(BF)

        @pl.when(step > 1)
        def _():
            swap_part(step - 2, span).wait_send()

        psend[lax.rem(step, 2)] = dot_nt(xgu[span, :], wgu[theirs, :]).astype(BF)
        swap_part(step, span).start()
        own[lax.rem(step, 2)] = dot_nt(xgu[span, :], wgu[mine, :])

    def quiet_backward(step, carry):
        backward(step, False)
        return carry

    def eager_backward(step, carry):
        backward(step, True)
        return carry

    def late_release(step, carry):
        release(step)
        return carry

    lax.fori_loop(0, deep, quiet_backward, 0)
    finish(deep - 1)
    lax.fori_loop(deep, PLANES, pass_rows, 0)
    lax.fori_loop(deep, PLANES, forward, 0)
    local_wait(near_bytes, bulk_sem.at[7])
    lax.fori_loop(deep, PLANES, eager_backward, 0)
    finish(PLANES - 1)
    release(PLANES - 1)
    lax.fori_loop(0, deep, late_release, 0)

    def share(shift, carry):
        dest = zed * peers + lax.rem(pos + shift, peers)
        remote(
            mixer, plane_ref.at[aligned(pos, tokens)], bulk_sem.at[3], mixer_sem.at[0], sp=dest
        ).start()
        return carry

    lax.fori_loop(1, peers, share, 0)
    keep = pltpu.make_async_copy(mixer, plane_ref.at[aligned(pos, tokens)], mixer_sem.at[1])
    keep.start()

    out_load = pltpu.make_async_copy(out_w, wgu, load_sem.at[0])
    out_load.start()

    tile = 256

    def weigh(side):
        def weight_tile(step, carry):
            columns = aligned(step, tile)
            spot = pl.ds(pl.multiple_of(side * half + step * tile, tile), tile)
            both = dot_tn(rows[side, :, columns], xgu[...]).astype(BF)
            gate_g[spot, :] = both[:, :hidden]
            up_g[spot, :] = both[:, hidden:]
            down_g[:, spot] = dot_tn(hid[...], grads[side, :, columns]).astype(BF)
            return carry

        lax.fori_loop(0, half // tile, weight_tile, 0)

    weigh(0)

    def gather(step, carry):
        kind, level = step // deep, lax.rem(step, deep)
        local_wait(back.at[kind, aligned(level, group)], back_sem.at[step])
        return carry

    lax.fori_loop(deep, PLANES, gather, 0)
    far_tok[...] = dot_tn(table[1], back[1]).astype(BF)
    far_sum = remote(far_tok, far_moe, far_send.at[4], far_recv.at[4], sp=far)
    far_sum.start()
    weigh(1)
    for slot in range(2 * PLANES):
        to_pair(rows.at[0, pl.ds(0, group)], slot).wait_send()
    shared = plane_ref.at[pl.ds(0, (peers - 1) * tokens)]
    local_wait(shared, mixer_sem.at[0])
    keep.wait()
    local_wait(shared, bulk_sem.at[3])
    chunks = peers * tokens // slots
    mixer_loads = [
        pltpu.make_async_copy(
            plane_ref.at[pl.ds(chunk * slots, slots)], rg.at[chunk], load_sem.at[1 + chunk]
        )
        for chunk in range(chunks)
    ]
    for load in mixer_loads:
        load.start()

    lax.fori_loop(0, deep, gather, 0)
    moe = dot_tn(table[0], back[0]) + near_cot[...].astype(F32)
    far_sum.wait_recv()
    halves[core] = (moe + far_moe[...].astype(F32)).astype(BF)
    last = to_pair(halves.at[core], 3 * PLANES)
    last.start()

    cut = width // count
    lane = cols.shape[1] // PLANES

    def column_block(level, place):
        return aligned((level * peers + place) * cut // lane, lane)

    def send_cols(shift, carry):
        place = lax.rem(pos + shift, peers)
        for level in range(deep):
            remote(
                halves.at[core, :, column_block(level, place)],
                cols.at[aligned(pos, tokens), aligned(core * deep + level, lane)],
                bulk_sem.at[4], cols_sem.at[0], sp=zed * peers + place,
            ).start()
        return carry

    lax.fori_loop(1, peers, send_cols, 0)
    kept = [
        pltpu.make_async_copy(
            halves.at[core, :, column_block(level, pos)],
            cols.at[aligned(pos, tokens), aligned(core * deep + level, lane)],
            cols_sem.at[1 + level],
        )
        for level in range(deep)
    ]
    for copy in kept:
        copy.start()

    grad_ref[:, mine] = halves[core]
    out_load.wait()
    to_pair(halves.at[other], 3 * PLANES).wait_recv()
    grad_ref[:, theirs] = halves[other]

    mixer_grad = dot_nn(halves[0], wgu[:half, :]) + dot_nn(halves[1], wgu[half:, :])
    gate_out[...] = (mixer_grad * slope[...]).astype(BF)
    for block in range(blocks):
        at = pl.ds(block * LANES, LANES)
        local[block] = mixer_grad[:, block * LANES : (block + 1) * LANES] * gelu[:, at]

    def scan(step, carry):
        picked = pl.ds(segment_rows - 1 - step, SEGMENTS, stride=segment_rows)
        after = []
        for block in range(blocks):
            total, decay = carry[block]
            total = local[block, picked, :] + decay * total
            local[block, picked, :] = total
            after.append((total, decays[block, picked, :]))
        return after

    picked = pl.ds(segment_rows - 1, SEGMENTS, stride=segment_rows)
    start = [(local[block, picked, :], decays[block, picked, :]) for block in range(blocks)]
    ended = lax.fori_loop(1, segment_rows, scan, start)
    total = jnp.concatenate([piece[0] * piece[1] for piece in ended], axis=1)
    product = products[...]
    whole, entry = product[SEGMENTS - 1 :], total[SEGMENTS - 1 :]
    for segment in range(SEGMENTS - 2, -1, -1):
        row = slice(segment, segment + 1)
        whole = whole * product[row]
        entry = total[row] + product[row] * entry
    pieces[pos, 0:1, :] = whole
    pieces[pos, 1:2, :] = entry

    def send_carry(shift, carry):
        dest = zed * peers + lax.rem(pos + shift, peers)
        remote(pieces.at[pos], pieces.at[pos], bulk_sem.at[6], carry_recv.at[pos], sp=dest).start()
        return carry

    lax.fori_loop(1, peers, send_carry, 0)

    local_wait(cols.at[pl.ds(0, (peers - 1) * tokens), pl.ds(0, deep * lane)], cols_sem.at[0])
    for copy in kept:
        copy.wait()
    cols_mine = cols.at[:, aligned(core, deep * lane)]
    cols_pass = to_pair(cols_mine, 3 * PLANES + 1)
    cols_pass.start()

    def wait_carry(shift, carry):
        source = lax.rem(pos + shift, peers)
        local_wait(pieces.at[source], carry_recv.at[source])
        return carry

    lax.fori_loop(1, peers, wait_carry, 0)
    blank = whole * 0.0
    whole, entry = blank + 1.0, blank
    after, after_entry = whole, entry
    for spot in range(peers - 1, -1, -1):
        factor, addend = pieces[spot, 0:1, :], pieces[spot, 1:2, :]
        whole = factor * whole
        entry = addend + factor * entry
        later = spot > pos
        after = jnp.where(later, factor * after, after)
        after_entry = jnp.where(later, addend + factor * after_entry, after_entry)
    plane_pair[0:1, :] = whole
    plane_pair[1:2, :] = entry

    def plane_copy(plane):
        return remote(
            plane_pair, plane_pieces.at[zed], plane_send.at[plane], plane_recv.at[zed],
            sp=plane * peers + pos,
        )

    def send_plane(step, carry):
        plane_copy(zed - 1 - step).start()
        return carry

    lax.fori_loop(0, zed, send_plane, 0)

    for load in mixer_loads:
        load.wait()
    to_pair(cols.at[:, aligned(other, deep * lane)], 3 * PLANES + 1).wait_recv()
    sums = pl.ds(0, PLANES * lane)
    partial = dot_tn(cols[pl.ds(0, slots), :], rg[0])
    for chunk in range(1, chunks):
        partial = partial + dot_tn(cols[pl.ds(chunk * slots, slots), :], rg[chunk])
    pre[sums, :] = partial
    send_part[...] = partial.astype(BF)

    def part_rows(plane):
        offset = lax.rem((plane * peers + pos) * cut, lane)
        return pl.ds(pl.multiple_of(plane * lane + offset, cut), cut)

    def send_block(shift, carry):
        plane = lax.rem(zed + shift, PLANES)
        remote(
            send_part.at[part_rows(plane)], got_part.at[aligned(zed, cut)],
            bulk_sem.at[5], part_sem.at[zed], sp=plane * peers + pos,
        ).start()
        return carry

    lax.fori_loop(1, PLANES, send_block, 0)

    def take_plane(step, entering):
        source = PLANES - 1 - step
        local_wait(plane_pieces.at[source], plane_recv.at[source])
        return plane_pieces[source, 0:1, :] * entering + plane_pieces[source, 1:2, :]

    entering = lax.fori_loop(0, PLANES - 1 - zed, take_plane, blank)
    entering = after_entry + after * entering
    enter = []
    for segment in range(SEGMENTS - 1, -1, -1):
        enter.append(entering)
        row = slice(segment, segment + 1)
        entering = total[row] + product[row] * entering
    enter = jnp.concatenate(enter[::-1], axis=0)

    for block in range(blocks):
        at = slice(block * LANES, (block + 1) * LANES)
        filled = jnp.broadcast_to(enter[:, None, at], (SEGMENTS, segment_rows, LANES))
        carried = local[block] + cumul[block] * filled.reshape(tokens, LANES)
        both = jnp.concatenate(
            [(carried * first[:, at]).astype(BF), (carried * second[:, at]).astype(BF)], axis=1
        )
        maps = jnp.concatenate([decay_w[block], input_w[block]], axis=1)
        conv_grad[0:tokens, at] = carried * third[:, at] + dot_nt(both, maps)

    halo = pl.ds(16, 8)
    halo_copy = remote(
        conv_grad.at[pl.ds(0, 8)], edge.at[halo], halo_sem.at[0], halo_sem.at[1], sp=me - 1
    )

    @pl.when(me > 0)
    def _():
        halo_copy.start()

    @pl.when(me == count - 1)
    def _():
        edge[halo, :] = jnp.zeros((8, channels), F32)

    edge[0:16, :] = conv_grad[tokens - 16 : tokens, :]

    def taps_over(source, rows):
        total = taps_ref[0:1, :] * source[3 : rows + 3, :]
        for tap in range(1, 4):
            total = total + taps_ref[tap : tap + 1, :] * source[3 - tap : rows + 3 - tap, :]
        return total.astype(BF)

    recur_out[0 : tokens - 16, :] = taps_over(conv_grad, tokens - 16)

    @pl.when(me < count - 1)
    def _():
        local_wait(edge.at[halo], halo_sem.at[1])

    recur_out[tokens - 16 : tokens, :] = taps_over(edge, 16)

    summed = pre[part_rows(zed), :]
    for shift in range(1, PLANES):
        plane = lax.rem(zed + shift, PLANES)
        local_wait(got_part.at[aligned(plane, cut)], part_sem.at[plane])
        summed = summed + got_part[aligned(plane, cut), :].astype(F32)
    weight_out[...] = summed

    for which in (1, 2):
        local_wait(sent_bytes, bulk_sem.at[which])
    local_wait(pieces.at[pl.ds(0, peers - 1)], bulk_sem.at[6])
    for copy in to_far:
        copy.wait_send()
    far_sum.wait_send()
    local_wait(cols.at[pl.ds(0, (peers - 1) * tokens), pl.ds(0, deep * lane)], bulk_sem.at[4])
    local_wait(got_part.at[pl.ds(0, (PLANES - 1) * cut)], bulk_sem.at[5])
    for step in range(PLANES - 2, PLANES):
        swap_part(step, pl.ds(0, group)).wait_send()
    last.wait_send()
    cols_pass.wait_send()

    def sent_plane(step, carry):
        plane_copy(zed - 1 - step).wait_send()
        return carry

    lax.fori_loop(0, zed, sent_plane, 0)

    @pl.when(me > 0)
    def _():
        halo_copy.wait_send()

    @pl.when(me < count - 1)
    def _():
        for copy in before:
            copy.wait_send()


def flush_kernel(total, *refs):
    sems = refs[-1]
    copies = [
        pltpu.make_async_copy(refs[item], refs[total + item], sems.at[item])
        for item in range(total)
    ]
    for copy in copies:
        copy.start()
    for copy in copies:
        copy.wait()


def flushed(*results):
    total = len(results)
    size = sum(result.size * result.dtype.itemsize for result in results)
    return pl.pallas_call(
        functools.partial(flush_kernel, total),
        in_specs=[pl.BlockSpec(memory_space=pltpu.VMEM)] * total,
        out_specs=[pl.BlockSpec(memory_space=pl.ANY)] * total,
        out_shape=[jax.ShapeDtypeStruct(result.shape, result.dtype) for result in results],
        scratch_shapes=[pltpu.SemaphoreType.DMA((total,))],
        compiler_params=pltpu.CompilerParams(vmem_limit_bytes=4 * 1024 * 1024),
        cost_estimate=pl.CostEstimate(flops=1000, bytes_accessed=2 * size, transcendentals=0),
        name="flush",
    )(*results)


def on_device(
    moe_input,
    cotangent,
    expert_ids,
    route_weight,
    gate_proj,
    up_proj,
    down_proj,
    out_weight,
    recur_input,
    gate_input,
    states,
    conv_taps,
    decay_gate_w,
    input_gate_w,
    decay_rate,
    decay_extra,
):
    count = lax.axis_size("sp")
    tokens, width = moe_input.shape
    cap = max(2, 4 * tokens // count)
    slots = count * cap
    half = width // 2
    hidden = gate_proj.shape[2]
    channels = states.shape[1]
    peers = count // PLANES
    group = peers * cap
    cut = width // count
    lane = max(cut, LANES)
    blocks = channels // LANES
    vmem, anywhere = pl.BlockSpec(memory_space=pltpu.VMEM), pl.BlockSpec(memory_space=pl.ANY)
    dma = pltpu.SemaphoreType.DMA

    def out(shape, kind):
        return pltpu.VMEM(shape, kind)

    def plain(kind):
        return pltpu.VMEM((tokens, channels), kind)

    results = pl.pallas_call(
        functools.partial(whole_kernel, count, cap),
        in_specs=[anywhere] * 2 + [vmem] * 6 + [anywhere] * 8,
        out_specs=[vmem] * 7 + [anywhere],
        out_shape=[
            out((width, hidden), BF), out((width, hidden), BF), out((hidden, width), BF),
            out((cut, channels), F32), out((tokens, width), BF), out((tokens, channels), BF),
            out((tokens, channels), BF), jax.ShapeDtypeStruct((peers * tokens, channels), BF),
        ],
        scratch_shapes=[
            pltpu.VMEM((width, 2 * hidden), BF),
            pltpu.VMEM((hidden, width), BF),
            pltpu.VMEM((2, slots // 2, tokens), BF),
            pltpu.VMEM((2, slots // 2, 1), F32),
            pltpu.VMEM((tokens, half), BF),
            pltpu.VMEM((tokens, half), BF),
            pltpu.VMEM((tokens, half), BF),
            pltpu.VMEM((tokens, half), BF),
            pltpu.VMEM((2, tokens), jnp.int32),
            pltpu.VMEM((2, tokens), F32),
            pltpu.VMEM((tokens, half), BF),
            pltpu.VMEM((2, slots // 2, half), BF),
            pltpu.VMEM((2, slots // 2, half), BF),
            pltpu.VMEM((4, slots, half), BF),
            pltpu.VMEM((slots, 2 * hidden), F32),
            pltpu.VMEM((slots, hidden), BF),
            pltpu.VMEM((slots, 2 * hidden), BF),
            pltpu.VMEM((2, group, half), F32),
            pltpu.VMEM((2, group, half), BF),
            pltpu.VMEM((slots, half), BF),
            pltpu.VMEM((2, slots // 2, half), BF),
            pltpu.VMEM((2, tokens, half), BF),
            pltpu.VMEM((peers * tokens, PLANES * lane), BF),
            pltpu.VMEM((PLANES * lane, channels), BF),
            pltpu.VMEM((PLANES * cut, channels), BF),
            plain(F32), plain(F32), plain(F32), plain(F32), plain(F32),
            *[pltpu.VMEM((blocks, tokens, LANES), F32)] * 3,
            pltpu.VMEM((4, channels), F32),
            pltpu.VMEM((24, channels), F32),
            pltpu.VMEM((tokens + 8, LANES), F32),
            pltpu.VMEM((16, channels), BF),
            pltpu.VMEM((8, channels), F32),
            pltpu.VMEM((peers, 2, channels), F32),
            pltpu.VMEM((2, channels), F32),
            pltpu.VMEM((PLANES, 2, channels), F32),
            pltpu.VMEM((SEGMENTS, channels), F32),
            dma((9,)), dma((8,)), dma((PLANES,)), dma((PLANES,)), dma((PLANES,)), dma((2,)),
            dma((3 * PLANES + 2,)), dma((3 * PLANES + 2,)), dma((4,)), dma((3,)), dma((PLANES,)),
            dma((peers,)), dma((PLANES,)), dma((PLANES,)), dma((2,)), dma((5,)), dma((5,)),
        ],
        compiler_params=pltpu.CompilerParams(
            collective_id=0, has_side_effects=True, vmem_limit_bytes=54 * 1024 * 1024
        ),
        cost_estimate=pl.CostEstimate(
            flops=16 * slots * width * hidden, bytes_accessed=40 << 20, transcendentals=0
        ),
        name="whole",
    )(
        moe_input, cotangent, expert_ids.T, route_weight.T, decay_gate_w, input_gate_w,
        conv_taps, decay_rate[None], gate_proj[0], up_proj[0], down_proj[0], out_weight,
        recur_input, gate_input, states, decay_extra,
    )
    gate_g, up_g, down_g, weight_g, grad, recur_g, gate_in_g = flushed(*results[:7])
    return (gate_g[None], up_g[None], down_g[None], weight_g, grad, recur_g, gate_in_g)


def solution(mesh):
    return jax.shard_map(
        on_device,
        mesh=mesh,
        in_specs=(
            P("sp", None),
            P("sp", None),
            P("sp", None),
            P("sp", None),
            P("sp", None, "tp"),
            P("sp", None, "tp"),
            P("sp", "tp", None),
            P(None, "tp"),
            P("sp", "tp"),
            P("sp", "tp"),
            P("sp", "tp"),
            P(None, "tp"),
            P("tp", None, None),
            P("tp", None, None),
            P("tp"),
            P("sp", "tp"),
        ),
        out_specs=(
            P("sp", None, "tp"),
            P("sp", None, "tp"),
            P("sp", "tp", None),
            P("sp", "tp"),
            P("sp", None),
            P("sp", "tp"),
            P("sp", "tp"),
        ),
        check_vma=False,
    )
```
